512 devices in a mesh: fs: 16 (over y, x), tp: 32 (over z, core).
Axes of the slice: x: 4, y: 4, z: 16, core: 2. Of those that a mesh axis runs over, the one named last changes fastest.
Arguments:
- x_later: bfloat16 [6144, 2048], P('fs'), may hold values from -6 to 6
- x_earlier: bfloat16 [6144, 2048], P('fs'), may hold values from -6 to 6
- cot_hidden: bfloat16 [6144, 4096], P('fs', 'tp'), may hold values from -6 to 6
- w_gate: bfloat16 [2048, 4096], P('fs', 'tp'), may hold values from -0.125 to 0.125
- w_up: bfloat16 [2048, 4096], P('fs', 'tp'), may hold values from -0.125 to 0.125
- grad_gate: float32 [2048, 4096], P('fs', 'tp'), may hold values from -192 to 192
- grad_up: float32 [2048, 4096], P('fs', 'tp'), may hold values from -192 to 192
Outputs:
- hidden_later: bfloat16 [6144, 4096], P('fs', 'tp')
- grad_input: bfloat16 [6144, 2048], P('fs')
- new_grad_gate: float32 [2048, 4096], P('fs', 'tp')
- new_grad_up: float32 [2048, 4096], P('fs', 'tp')
The draws below stay inside these ranges and needn't reach their ends.
All inputs are finite; a program needn't handle non-finite values.
Results may differ from the reference program's by a relative error of at most 0.018.
Values may be sent and summed in bfloat16 or wider, within the bound.
A program may use at most 64 MiB of HBM per device.

```python
import jax
import jax.numpy as jnp
from jax import lax

D = 2048
FF = 4096
TOKENS = 6144
N_TP = 32


def raised(entries, stream_key, source, target, parts, factor):
    owner, partner = [(jnp.arange(entries.shape[axis_at]) // (entries.shape[axis_at] // parts)).reshape([-1 if axis == axis_at else 1 for axis in range(entries.ndim)]) for axis_at in (source, target)]
    chosen = jax.random.permutation(stream_key, parts)[partner]
    strong = (owner == chosen) | (owner == (partner + parts // 2) % parts)
    return jnp.where(strong, factor * entries, entries)


def steps_of(rng, shape, cuts, low, top_value):
    level, own = 1.0, jax.random.fold_in(rng, 6)
    for dim, blocks in cuts:
        draws = jnp.exp(jax.random.uniform(jax.random.fold_in(own, dim), (blocks,), jnp.float32, low / len(cuts), top_value / len(cuts)))
        level = level * jnp.repeat(draws, shape[dim] // blocks).reshape([-1 if axis == dim else 1 for axis in range(len(shape))])
    return level


def centred(key, shape, scale, most, cuts=(), held_as=jnp.bfloat16):
    array = scale * jax.random.normal(key, shape, jnp.float32)
    if cuts:
        array = array * steps_of(key, shape, cuts, -0.22, 0.18)
    return jnp.clip(array, -most, most).astype(held_as)


def gaussian_with(own_key, dims, deviation, limit, pieces, heavy, kind=jnp.bfloat16):
    entries = deviation * jax.random.normal(own_key, dims, jnp.float32)
    if pieces:
        entries = entries * steps_of(own_key, dims, pieces, -0.22, 0.18)
    return jnp.clip(raised(entries, jax.random.fold_in(own_key, 3), *heavy), -limit, limit).astype(kind)


def setup_inputs(seed: int = 0) -> dict:
    key_list = jax.random.split(jax.random.key(seed), 8)
    return {
        "x_later": centred(key_list[0], (TOKENS, D), 1.0, 6.0, ((0, 16),)),
        "x_earlier": gaussian_with(key_list[1], (TOKENS, D), 1.0, 6.0, ((0, 16),), (0, 1, 16, 2.0)),
        "cot_hidden": gaussian_with(key_list[2], (TOKENS, FF), 1.0, 6.0, ((0, 16), (1, 32)), (1, 0, 32, 2.75)),
        "w_gate": centred(key_list[3], (D, FF), D ** -0.5, 0.125, ((0, 16), (1, 32))),
        "w_up": centred(key_list[4], (D, FF), D ** -0.5, 0.125, ((0, 16), (1, 32))),
        "grad_gate": centred(key_list[5], (D, FF), 32.0, 192.0, ((0, 16), (1, 32)), jnp.float32),
        "grad_up": centred(key_list[6], (D, FF), 32.0, 192.0, ((0, 16), (1, 32)), jnp.float32),
    }


def reference(x_later, x_earlier, cot_hidden, w_gate, w_up, grad_gate, grad_up):
    gate_later = jnp.dot(x_later, w_gate, preferred_element_type=jnp.float32)
    up_later = jnp.dot(x_later, w_up, preferred_element_type=jnp.float32)
    hidden_later = (jax.nn.silu(gate_later) * up_later).astype(jnp.bfloat16)
    gate_earlier = jnp.dot(x_earlier, w_gate, preferred_element_type=jnp.float32)
    up_earlier = jnp.dot(x_earlier, w_up, preferred_element_type=jnp.float32)
    sigma = jax.nn.sigmoid(gate_earlier)
    cotangent = cot_hidden.astype(jnp.float32)
    delta_up = (cotangent * gate_earlier * sigma).astype(jnp.bfloat16)
    delta_gate = (cotangent * up_earlier * sigma * (1.0 + gate_earlier * (1.0 - sigma))).astype(jnp.bfloat16)
    width = FF // N_TP

    def add_block(total, index):
        offset = (index * width).astype(jnp.int32)
        block_gate = lax.dynamic_slice_in_dim(delta_gate, offset, width, 1)
        block_up = lax.dynamic_slice_in_dim(delta_up, offset, width, 1)
        weight_gate = lax.dynamic_slice_in_dim(w_gate, offset, width, 1)
        weight_up = lax.dynamic_slice_in_dim(w_up, offset, width, 1)
        partial_value = jnp.dot(block_gate, weight_gate.T, preferred_element_type=jnp.float32)
        partial_value = partial_value + jnp.dot(block_up, weight_up.T, preferred_element_type=jnp.float32)
        rounded = lax.optimization_barrier(partial_value.astype(jnp.bfloat16))
        return total + rounded.astype(jnp.float32), None

    summed, _ = lax.scan(add_block, jnp.zeros(x_earlier.shape, jnp.float32), jnp.arange(N_TP, dtype=jnp.int32))
    grad_input = summed.astype(jnp.bfloat16)
    new_grad_gate = grad_gate + jnp.dot(x_earlier.T, delta_gate, preferred_element_type=jnp.float32)
    new_grad_up = grad_up + jnp.dot(x_earlier.T, delta_up, preferred_element_type=jnp.float32)
    return hidden_later, grad_input, new_grad_gate, new_grad_up
```

```python
import functools

import jax
import jax.numpy as jnp
from jax import lax
from jax.experimental import pallas as pl
from jax.experimental.pallas import tpu as pltpu
from jax.sharding import PartitionSpec as P

MESH = pl.DeviceIdType.MESH
SUB = 2
F32 = jnp.float32
BF16 = jnp.bfloat16


def kernel(
    nz,
    xl_h, xe_h, cot_h, wg_h, wu_h, gg_h, gu_h, hid_o, gi_o, ngg_o, ngu_o,
    xl, xe, cot, gg, gu, hid, ngg, ngu,
    wq, wall,
    dcat, dwt, dwr, dw_own,
    pc, ps, pown, sp, sm, rp, rm, gi,
    in_sem, out_sem, gi_out_sem,
    ag_send, ag_recv, dw_send, dw_recv, ps_send, ps_recv,
    rsp_send, rsp_recv, rsm_send, rsm_recv,
    agp_send, agp_recv, agm_send, agm_recv, d2_send, d2_recv,
):
    rows = xe.shape[0]
    blocks = xe.shape[1] // 128
    up = nz // 2
    dn = nz - 1 - up
    per = blocks // nz
    crows = per * rows
    piece = crows // SUB

    f = lax.axis_index("fs")
    t = lax.axis_index("tp")
    y, x = f // 4, f % 4
    z, core = t // 2, t % 2

    loads = [
        pltpu.make_async_copy(wg_h, wq.at[:, 0, :, pl.ds(0, 128)], in_sem.at[0]),
        pltpu.make_async_copy(wu_h, wq.at[:, 0, :, pl.ds(128, 128)], in_sem.at[1]),
        pltpu.make_async_copy(xe_h, xe, in_sem.at[2]),
        pltpu.make_async_copy(cot_h, cot, in_sem.at[3]),
        pltpu.make_async_copy(xl_h, xl, in_sem.at[4]),
        pltpu.make_async_copy(gg_h, gg, in_sem.at[5]),
        pltpu.make_async_copy(gu_h, gu, in_sem.at[6]),
    ]
    for load in loads:
        load.start()

    x1 = x + 1 - 2 * (x % 2)
    y1 = y + 1 - 2 * (y % 2)
    flips = [y * 4 + x1, y * 4 + (3 - x), y1 * 4 + x, (3 - y) * 4 + x]
    right = {"fs": f, "tp": ((z + 1) % nz) * 2 + core}
    left = {"fs": f, "tp": ((z + nz - 1) % nz) * 2 + core}
    partner = {"fs": f, "tp": z * 2 + 1 - core}

    barrier = pltpu.get_barrier_semaphore()
    for g in flips:
        pl.semaphore_signal(barrier, inc=1, device_id={"fs": g, "tp": t}, device_id_type=MESH)
    for who in (partner, right, left):
        pl.semaphore_signal(barrier, inc=1, device_id=who, device_id_type=MESH)
    pl.semaphore_wait(barrier, 7)

    def gather_send(q, s, first, count):
        pltpu.make_async_remote_copy(
            src_ref=wq.at[q, pl.ds(first, count)],
            dst_ref=wq.at[q, pl.ds(first + 2**s, count)],
            send_sem=ag_send,
            recv_sem=ag_recv.at[q, s],
            device_id={"fs": flips[(q + s) % 4], "tp": t},
            device_id_type=MESH,
        ).start()

    def gather_wait(q, s):
        got = wq.at[q, pl.ds(2**s, 2**s)]
        pltpu.make_async_copy(got, got, ag_recv.at[q, s]).wait()

    loads[0].wait()
    loads[1].wait()
    for s in range(4):
        for q in range(4):
            gather_send(q, s, 0, 1)
    for a in range(3):
        for q in range(4):
            gather_wait(q, a)
            for s in range(a + 1, 4):
                gather_send(q, s, 2**a, 2**a)
    for q in range(4):
        gather_wait(q, 3)

    for q in range(4):
        for i in range(16):
            bits = [(q + b) % 4 for b in range(4) if (i >> b) & 1]
            ox = x
            oy = y
            if 0 in bits:
                ox = ox + 1 - 2 * (ox % 2)
            if 1 in bits:
                ox = 3 - ox
            if 2 in bits:
                oy = oy + 1 - 2 * (oy % 2)
            if 3 in bits:
                oy = 3 - oy
            start = pl.multiple_of((oy * 4 + ox) * 128 + 32 * q, 32)
            wall[pl.ds(start, 32), :] = wq[q, i]

    loads[2].wait()
    loads[3].wait()
    both = jnp.dot(xe[...], wall[...], preferred_element_type=F32)
    gate, upv = both[:, :128], both[:, 128:]
    sigma = jax.nn.sigmoid(gate)
    cotangent = cot[...].astype(F32)
    delta_up = cotangent * gate * sigma
    delta_gate = cotangent * upv * sigma * (1.0 + gate * (1.0 - sigma))
    dcat[:, pl.ds(0, 128)] = delta_gate.astype(BF16)
    dcat[:, pl.ds(128, 128)] = delta_up.astype(BF16)

    def partial_block(d, b):
        first = pl.multiple_of((d * per + b) * 128, 128)
        return lax.dot_general(
            dcat[...], wall[pl.ds(first, 128), :], (((1,), (1,)), ((), ())),
            preferred_element_type=F32,
        )

    def weight_gradients():
        turned = jnp.transpose(dcat[...].astype(F32)).astype(BF16)
        for i in range(16):
            to = (f + i) % 16
            first = pl.multiple_of(to * 128, 128)
            block = jnp.dot(turned, xe[:, pl.ds(first, 128)], preferred_element_type=F32)
            if i == 0:
                dw_own[...] = block
            else:
                dwt[i - 1] = block.astype(BF16)
                pltpu.make_async_remote_copy(
                    src_ref=dwt.at[i - 1],
                    dst_ref=dwr.at[i - 1],
                    send_sem=dw_send,
                    recv_sem=dw_recv.at[i - 1],
                    device_id={"fs": to, "tp": t},
                    device_id_type=MESH,
                ).start()

    def weight_gradients_done():
        total = dw_own[...]
        for i in range(15):
            pltpu.make_async_copy(dwr.at[i], dwr.at[i], dw_recv.at[i]).wait()
            total = total + dwr[i].astype(F32)
        loads[5].wait()
        loads[6].wait()
        ngg[...] = gg[...] + jnp.transpose(total[:128])
        ngu[...] = gu[...] + jnp.transpose(total[128:])
        pltpu.make_async_copy(ngg, ngg_o, out_sem.at[0]).start()
        pltpu.make_async_copy(ngu, ngu_o, out_sem.at[1]).start()

    def later():
        loads[4].wait()
        both = jnp.dot(xl[...], wall[...], preferred_element_type=F32)
        gate, upv = both[:, :128], both[:, 128:]
        hid[...] = (gate * jax.nn.sigmoid(gate) * upv).astype(BF16)
        pltpu.make_async_copy(hid, hid_o, out_sem.at[2]).start()

    def put_out(o):
        for b in range(per):
            first = pl.multiple_of((o * per + b) * 128, 128)
            pltpu.make_async_copy(
                gi.at[o, pl.ds(b * rows, rows)], gi_o.at[:, pl.ds(first, 128)], gi_out_sem
            ).start()

    def at(k):
        return pl.ds(k * piece, piece)

    @pl.when(core == 0)
    def _():
        def give(d):
            for b in range(per):
                pown[d, pl.ds(b * rows, rows)] = partial_block(d, b).astype(BF16)
            pltpu.make_async_remote_copy(
                src_ref=pown.at[d], dst_ref=ps.at[d], send_sem=ps_send, recv_sem=ps_recv.at[d],
                device_id=partner, device_id_type=MESH,
            ).start()

        for s in range(up):
            give((z + up - s) % nz)
            if s < dn:
                give((z + nz - dn + s) % nz)
        give(z)
        weight_gradients()
        later()
        weight_gradients_done()
        order = [z]
        for s in range(1, up + 1):
            order.append((z + nz - s) % nz)
            if s <= dn:
                order.append((z + s) % nz)
        for o in order:
            for k in range(SUB):
                pltpu.make_async_copy(gi.at[o, at(k)], gi.at[o, at(k)], d2_recv.at[o, k]).wait()
            put_out(o)
        pltpu.make_async_copy(pown, pown, ps_send).wait()

    @pl.when(core == 1)
    def _():
        def take(d):
            for b in range(per):
                pc[d, pl.ds(b * rows, rows)] = partial_block(d, b)
            pltpu.make_async_copy(ps.at[d], ps.at[d], ps_recv.at[d]).wait()
            pc[d] = pc[d] + ps[d].astype(F32)

        def forward(src, dst, send_sem, recv_sem, who):
            pltpu.make_async_remote_copy(
                src_ref=src, dst_ref=dst, send_sem=send_sem, recv_sem=recv_sem,
                device_id=who, device_id_type=MESH,
            ).start()

        def arrived(ref, sem):
            pltpu.make_async_copy(ref, ref, sem).wait()

        take((z + up) % nz)
        if dn > 0:
            take((z + nz - dn) % nz)
        for s in range(up):
            for k in range(SUB):
                value = pc[(z + up - s) % nz, at(k)]
                if s > 0:
                    arrived(rp.at[s - 1, at(k)], rsp_recv.at[s - 1, k])
                    value = value + rp[s - 1, at(k)].astype(F32)
                sp[s, at(k)] = value.astype(BF16)
                forward(sp.at[s, at(k)], rp.at[s, at(k)], rsp_send, rsp_recv.at[s, k], right)
                if s < dn:
                    value = pc[(z + nz - dn + s) % nz, at(k)]
                    if s > 0:
                        arrived(rm.at[s - 1, at(k)], rsm_recv.at[s - 1, k])
                        value = value + rm[s - 1, at(k)].astype(F32)
                    sm[s, at(k)] = value.astype(BF16)
                    forward(sm.at[s, at(k)], rm.at[s, at(k)], rsm_send, rsm_recv.at[s, k], left)
            if s + 1 < up:
                take((z + up - s - 1) % nz)
            else:
                take(z)
            if s + 1 < dn:
                take((z + nz - dn + s + 1) % nz)
            if s == min(2, up - 1):
                weight_gradients()

        for k in range(SUB):
            value = pc[z, at(k)]
            arrived(rp.at[up - 1, at(k)], rsp_recv.at[up - 1, k])
            value = value + rp[up - 1, at(k)].astype(F32)
            if dn > 0:
                arrived(rm.at[dn - 1, at(k)], rsm_recv.at[dn - 1, k])
                value = value + rm[dn - 1, at(k)].astype(F32)
            gi[z, at(k)] = value.astype(BF16)
            mine = gi.at[z, at(k)]
            forward(mine, mine, agp_send, agp_recv.at[0, k], right)
            if dn > 0:
                forward(mine, mine, agm_send, agm_recv.at[0, k], left)
            forward(mine, mine, d2_send, d2_recv.at[z, k], partner)
        put_out(z)

        for s in range(1, up + 1):
            low = (z + nz - s) % nz
            high = (z + s) % nz
            for k in range(SUB):
                part = gi.at[low, at(k)]
                arrived(part, agp_recv.at[s - 1, k])
                if s < up:
                    forward(part, part, agp_send, agp_recv.at[s, k], right)
                forward(part, part, d2_send, d2_recv.at[low, k], partner)
                if s <= dn:
                    part = gi.at[high, at(k)]
                    arrived(part, agm_recv.at[s - 1, k])
                    if s < dn:
                        forward(part, part, agm_send, agm_recv.at[s, k], left)
                    forward(part, part, d2_send, d2_recv.at[high, k], partner)
            put_out(low)
            if s <= dn:
                put_out(high)
            if s == 1:
                later()
            if s == min(3, up):
                weight_gradients_done()

        arrived(sp, rsp_send)
        arrived(gi.at[pl.ds(0, up)], agp_send)
        if dn > 0:
            arrived(sm.at[pl.ds(0, dn)], rsm_send)
            arrived(gi.at[pl.ds(0, dn)], agm_send)
        arrived(gi, d2_send)

    pltpu.make_async_copy(wq.at[:, pl.ds(0, 15)], wq.at[:, pl.ds(0, 15)], ag_send).wait()
    pltpu.make_async_copy(dwt, dwt, dw_send).wait()
    pltpu.make_async_copy(gi, gi, gi_out_sem).wait()
    pltpu.make_async_copy(ngg, ngg_o, out_sem.at[0]).wait()
    pltpu.make_async_copy(ngu, ngu_o, out_sem.at[1]).wait()
    pltpu.make_async_copy(hid, hid_o, out_sem.at[2]).wait()


def per_device(nz, x_later, x_earlier, cot_hidden, w_gate, w_up, grad_gate, grad_up):
    rows, width = x_later.shape
    up = nz // 2
    dn = nz - 1 - up
    crows = (width // 128 // nz) * rows
    dma = pltpu.SemaphoreType.DMA
    any_spec = pl.BlockSpec(memory_space=pl.ANY)
    return pl.pallas_call(
        functools.partial(kernel, nz),
        out_shape=(
            jax.ShapeDtypeStruct((rows, 128), BF16),
            jax.ShapeDtypeStruct((rows, width), BF16),
            jax.ShapeDtypeStruct((128, 128), F32),
            jax.ShapeDtypeStruct((128, 128), F32),
        ),
        in_specs=[any_spec] * 7,
        out_specs=(any_spec,) * 4,
        scratch_shapes=[
            pltpu.VMEM((rows, width), BF16),
            pltpu.VMEM((rows, width), BF16),
            pltpu.VMEM((rows, 128), BF16),
            pltpu.VMEM((128, 128), F32),
            pltpu.VMEM((128, 128), F32),
            pltpu.VMEM((rows, 128), BF16),
            pltpu.VMEM((128, 128), F32),
            pltpu.VMEM((128, 128), F32),
            pltpu.VMEM((4, 16, 32, 256), BF16),
            pltpu.VMEM((width, 256), BF16),
            pltpu.VMEM((rows, 256), BF16),
            pltpu.VMEM((15, 256, 128), BF16),
            pltpu.VMEM((15, 256, 128), BF16),
            pltpu.VMEM((256, 128), F32),
            pltpu.VMEM((nz, crows, 128), F32),
            pltpu.VMEM((nz, crows, 128), BF16),
            pltpu.VMEM((nz, crows, 128), BF16),
            pltpu.VMEM((up, crows, 128), BF16),
            pltpu.VMEM((max(dn, 1), crows, 128), BF16),
            pltpu.VMEM((up, crows, 128), BF16),
            pltpu.VMEM((max(dn, 1), crows, 128), BF16),
            pltpu.VMEM((nz, crows, 128), BF16),
            dma((7,)),
            dma((3,)),
            dma,
            dma,
            dma((4, 4)),
            dma,
            dma((15,)),
            dma,
            dma((nz,)),
            dma,
            dma((up, SUB)),
            dma,
            dma((max(dn, 1), SUB)),
            dma,
            dma((up, SUB)),
            dma,
            dma((max(dn, 1), SUB)),
            dma,
            dma((nz, SUB)),
        ],
        compiler_params=pltpu.CompilerParams(
            collective_id=0, has_side_effects=True, vmem_limit_bytes=48 * 1024 * 1024
        ),
        name="step",
    )(
        x_later,
        x_earlier,
        cot_hidden,
        w_gate.reshape(4, 32, 128),
        w_up.reshape(4, 32, 128),
        grad_gate,
        grad_up,
    )


def solution(mesh):
    placed = (
        P("fs", None),
        P("fs", None),
        P("fs", "tp"),
        P("fs", "tp"),
        P("fs", "tp"),
        P("fs", "tp"),
        P("fs", "tp"),
    )
    return jax.shard_map(
        functools.partial(per_device, mesh.shape["tp"] // 2),
        mesh=mesh,
        in_specs=placed,
        out_specs=(P("fs", "tp"), P("fs", None), P("fs", "tp"), P("fs", "tp")),
        check_vma=False,
    )
```

```python
import functools

import jax
import jax.numpy as jnp
from jax import lax
from jax.experimental import pallas as pl
from jax.experimental.pallas import tpu as pltpu
from jax.sharding import PartitionSpec as P

MESH = pl.DeviceIdType.MESH
SUB = 2
F32 = jnp.float32
BF16 = jnp.bfloat16


def copy_to(src, dst, send_sem, recv_sem, who):
    pltpu.make_async_remote_copy(
        src_ref=src, dst_ref=dst, send_sem=send_sem, recv_sem=recv_sem,
        device_id=who, device_id_type=MESH,
    ).start()


def arrived(ref, sem):
    pltpu.make_async_copy(ref, ref, sem).wait()


def kernel(
    nz,
    xl_h, xe_h, cot_h, wg_h, wu_h, gg_h, gu_h, hid, gi, ngg, ngu,
    xl, xe, cot, gg, gu,
    wq, wall,
    dcat, dwt, dwr, hid_other,
    pc, ring_s, ring_r,
    in_sem, give_send, give_recv, ag_send, ag_recv,
    share_send, share_recv, dw_send, dw_recv, hid_send, hid_recv,
    rs_send, rs_recv, gather_send_sem, gather_recv, d2_send, d2_recv,
):
    rows = xe.shape[0]
    piece = rows // SUB
    half = nz // 2
    steps = nz // 4

    f = lax.axis_index("fs")
    t = lax.axis_index("tp")
    y, x = f // 4, f % 4
    z, core = t // 2, t % 2
    x1 = x + 1 - 2 * (x % 2)
    y1 = y + 1 - 2 * (y % 2)
    flips = [y * 4 + x1, y * 4 + (3 - x), y1 * 4 + x, (3 - y) * 4 + x]
    partner = {"fs": f, "tp": z * 2 + 1 - core}

    def along(by):
        return {"fs": f, "tp": ((z + nz + by) % nz) * 2 + core}

    def at(k):
        return pl.ds(k * piece, piece)

    load_xe = pltpu.make_async_copy(xe_h, xe, in_sem.at[0])
    load_gg = pltpu.make_async_copy(gg_h, gg, in_sem.at[1])
    load_gu = pltpu.make_async_copy(gu_h, gu, in_sem.at[2])
    barrier = pltpu.get_barrier_semaphore()

    def new_gradients(total):
        load_gg.wait()
        load_gu.wait()
        ngg[...] = gg[...] + jnp.transpose(total[:128])
        ngu[...] = gu[...] + jnp.transpose(total[128:])

    @pl.when(core == 0)
    def _():
        load_xl = pltpu.make_async_copy(xl_h, xl, in_sem.at[3])
        pl.semaphore_signal(barrier, inc=1, device_id=partner, device_id_type=MESH)
        pl.semaphore_wait(barrier, 1)
        copy_to(wg_h, wq.at[:, 0, :, pl.ds(0, 128)], give_send.at[0], give_recv.at[0], partner)
        copy_to(wu_h, wq.at[:, 0, :, pl.ds(128, 128)], give_send.at[1], give_recv.at[1], partner)
        copy_to(cot_h, cot.at[0], give_send.at[2], give_recv.at[2], partner)
        for load in (load_xe, load_xl, load_gg, load_gu):
            load.start()

        arrived(dcat, share_recv.at[0])
        load_xe.wait()
        turned = jnp.transpose(dcat[...].astype(F32)).astype(BF16)
        for j in range(4):
            block = jnp.dot(turned, xe[:, 512 * j : 512 * j + 512], preferred_element_type=F32)
            for i in range(4):
                dwt[4 * j + i] = block[:, 128 * i : 128 * i + 128].astype(BF16)
        copy_to(dwt.at[f, pl.ds(256, 256)], dwr.at[0], dw_send.at[1], dw_recv.at[0], partner)
        for i in range(1, 16):
            to = (f + i) % 16
            for c in range(2):
                copy_to(
                    dwt.at[to, pl.ds(256 * c, 256)], dwr.at[i], dw_send.at[0], dw_recv.at[i],
                    {"fs": to, "tp": z * 2 + c},
                )

        load_xl.wait()
        arrived(wall, share_recv.at[1])
        both = jnp.dot(xl[...], wall[...], preferred_element_type=F32)
        gate, upv = both[:, 256:384], both[:, 384:]
        hid_other[...] = (gate * jax.nn.sigmoid(gate) * upv).astype(BF16)
        gate, upv = both[:, :128], both[:, 128:256]
        hid[...] = (gate * jax.nn.sigmoid(gate) * upv).astype(BF16)

        total = dwt[f, pl.ds(0, 256)].astype(F32)
        copy_to(hid_other, hid, hid_send, hid_recv, partner)
        for i in range(1, 16):
            arrived(dwr.at[i], dw_recv.at[i])
            total = total + dwr[i].astype(F32)
        new_gradients(total)

        for k in range(SUB):
            arrived(gi.at[:, at(k)], d2_recv.at[k])
        pltpu.make_async_copy(wg_h, wg_h, give_send.at[0]).wait()
        pltpu.make_async_copy(wu_h, wu_h, give_send.at[1]).wait()
        pltpu.make_async_copy(cot_h, cot_h, give_send.at[2]).wait()
        arrived(hid_other, hid_send)
        arrived(dwt.at[pl.ds(0, 15)], dw_send.at[0])
        arrived(dwr.at[0], dw_send.at[1])

    @pl.when(core == 1)
    def _():
        load_wg = pltpu.make_async_copy(wg_h, wq.at[:, 0, :, pl.ds(256, 128)], in_sem.at[3])
        load_wu = pltpu.make_async_copy(wu_h, wq.at[:, 0, :, pl.ds(384, 128)], in_sem.at[4])
        load_cot = pltpu.make_async_copy(cot_h, cot.at[1], in_sem.at[5])
        pl.semaphore_signal(barrier, inc=1, device_id=partner, device_id_type=MESH)
        for g in flips:
            pl.semaphore_signal(barrier, inc=1, device_id={"fs": g, "tp": t}, device_id_type=MESH)
        for by in (-2, -1, 1, 2):
            pl.semaphore_signal(barrier, inc=1, device_id=along(by), device_id_type=MESH)
        for load in (load_wg, load_wu, load_xe, load_cot, load_gg, load_gu):
            load.start()
        pl.semaphore_wait(barrier, 9)

        def gather_send(q, s, first, count):
            copy_to(
                wq.at[q, pl.ds(first, count)], wq.at[q, pl.ds(first + 2**s, count)],
                ag_send, ag_recv.at[q, s], {"fs": flips[(q + s) % 4], "tp": t},
            )

        def gather_wait(q, s):
            arrived(wq.at[q, pl.ds(2**s, 2**s)], ag_recv.at[q, s])

        load_wg.wait()
        load_wu.wait()
        arrived(wq.at[:, 0, :, pl.ds(0, 128)], give_recv.at[0])
        arrived(wq.at[:, 0, :, pl.ds(128, 128)], give_recv.at[1])
        for s in range(4):
            for q in range(4):
                gather_send(q, s, 0, 1)
        for a in range(3):
            for q in range(4):
                gather_wait(q, a)
                for s in range(a + 1, 4):
                    gather_send(q, s, 2**a, 2**a)
        for q in range(4):
            gather_wait(q, 3)
        for q in range(4):
            for i in range(16):
                bits = [(q + b) % 4 for b in range(4) if (i >> b) & 1]
                ox = x
                oy = y
                if 0 in bits:
                    ox = ox + 1 - 2 * (ox % 2)
                if 1 in bits:
                    ox = 3 - ox
                if 2 in bits:
                    oy = oy + 1 - 2 * (oy % 2)
                if 3 in bits:
                    oy = 3 - oy
                start = pl.multiple_of((oy * 4 + ox) * 128 + 32 * q, 32)
                wall[pl.ds(start, 32), :] = wq[q, i]

        load_xe.wait()
        load_cot.wait()
        arrived(cot.at[0], give_recv.at[2])
        both = jnp.dot(xe[...], wall[...], preferred_element_type=F32)
        for c in range(2):
            gate = both[:, 256 * c : 256 * c + 128]
            upv = both[:, 256 * c + 128 : 256 * c + 256]
            sigma = jax.nn.sigmoid(gate)
            cotangent = cot[c].astype(F32)
            delta_up = cotangent * gate * sigma
            delta_gate = cotangent * upv * sigma * (1.0 + gate * (1.0 - sigma))
            dcat[:, 256 * c : 256 * c + 128] = delta_gate.astype(BF16)
            dcat[:, 256 * c + 128 : 256 * c + 256] = delta_up.astype(BF16)
        for j in range(4):
            block = lax.dot_general(
                dcat[...], wall[512 * j : 512 * j + 512, :], (((1,), (1,)), ((), ())),
                preferred_element_type=F32,
            )
            for i in range(4):
                pc[4 * j + i] = block[:, 128 * i : 128 * i + 128]

        def chunk(by):
            return (z + nz + by) % nz

        def ring(k, w):
            go = 1 if (k + w) % 2 == 0 else -1
            return go, half - w

        def reduce_step(i, k, w):
            go, length = ring(k, w)
            far, near = half - 2 * i, half - 2 * i - 1
            if far > 0 and far <= length:
                value = pc[chunk(go * far), at(k)]
                if i > 0:
                    arrived(ring_r.at[w, 1, i - 1, at(k)], rs_recv.at[k, w, 1, i - 1])
                    value = value + ring_r[w, 1, i - 1, at(k)].astype(F32)
                    if far + 2 <= length:
                        arrived(ring_r.at[w, 0, i - 1, at(k)], rs_recv.at[k, w, 0, i - 1])
                        value = value + ring_r[w, 0, i - 1, at(k)].astype(F32)
                part = ring_s.at[w, 0, i, at(k)]
                ring_s[w, 0, i, at(k)] = value.astype(BF16)
                copy_to(
                    part, ring_r.at[w, 0, i, at(k)], rs_send, rs_recv.at[k, w, 0, i], along(2 * go)
                )
            if near > 0:
                part = ring_s.at[w, 1, i, at(k)]
                ring_s[w, 1, i, at(k)] = pc[chunk(go * near), at(k)].astype(BF16)
                copy_to(part, ring_r.at[w, 1, i, at(k)], rs_send, rs_recv.at[k, w, 1, i], along(go))

        sent = 0
        for i in range(steps):
            for k in range(SUB):
                for w in range(2):
                    reduce_step(i, k, w)
            if i == 0:
                copy_to(dcat, dcat, share_send.at[0], share_recv.at[0], partner)
                copy_to(wall, wall, share_send.at[1], share_recv.at[1], partner)

        def spread(i, k, w, origin):
            go, length = ring(k, w)
            part = gi.at[origin, at(k)]
            if 2 * i + 2 <= length:
                copy_to(part, part, gather_send_sem, gather_recv.at[k, w, 0, i], along(2 * go))
            if 2 * i + 1 <= length:
                copy_to(part, part, gather_send_sem, gather_recv.at[k, w, 1, i], along(go))

        for k in range(SUB):
            value = pc[z, at(k)]
            for w in range(2):
                for hop in range(2):
                    arrived(ring_r.at[w, hop, steps - 1, at(k)], rs_recv.at[k, w, hop, steps - 1])
                    value = value + ring_r[w, hop, steps - 1, at(k)].astype(F32)
            gi[z, at(k)] = value.astype(BF16)
            for w in range(2):
                spread(0, k, w, z)
            copy_to(gi.at[z, at(k)], gi.at[z, at(k)], d2_send, d2_recv.at[k], partner)

        for i in range(steps):
            if i == steps - 1:
                total = jnp.zeros((256, 128), F32)
                for j in range(16):
                    arrived(dwr.at[j], dw_recv.at[j])
                    total = total + dwr[j].astype(F32)
                new_gradients(total)
            for k in range(SUB):
                for w in range(2):
                    go, length = ring(k, w)
                    if 2 * i + 1 <= length:
                        origin = chunk(-go * (2 * i + 1))
                        part = gi.at[origin, at(k)]
                        arrived(part, gather_recv.at[k, w, 1, i])
                        copy_to(part, part, d2_send, d2_recv.at[k], partner)
                    if 2 * i + 2 <= length:
                        origin = chunk(-go * (2 * i + 2))
                        part = gi.at[origin, at(k)]
                        arrived(part, gather_recv.at[k, w, 0, i])
                        if i + 1 < steps:
                            spread(i + 1, k, w, origin)
                        copy_to(part, part, d2_send, d2_recv.at[k], partner)

        arrived(hid, hid_recv)
        arrived(dcat, share_send.at[0])
        arrived(wall, share_send.at[1])
        arrived(wq.at[:, pl.ds(0, 15)], ag_send)
        arrived(gi, d2_send)
        arrived(gi.at[pl.ds(0, nz - 1)], rs_send)
        arrived(gi.at[pl.ds(0, nz - 1)], gather_send_sem)


def store(hid, gi, ngg, ngu, hid_o, gi_o, ngg_o, ngu_o, hid_sem, gi_sem, ngg_sem, ngu_sem):
    for o in range(gi.shape[0]):
        pltpu.make_async_copy(gi.at[o], gi_o.at[:, pl.ds(o * 128, 128)], gi_sem).start()
    small = [
        pltpu.make_async_copy(hid, hid_o, hid_sem),
        pltpu.make_async_copy(ngg, ngg_o, ngg_sem),
        pltpu.make_async_copy(ngu, ngu_o, ngu_sem),
    ]
    for copy in small:
        copy.start()
    for copy in small:
        copy.wait()
    pltpu.make_async_copy(gi, gi, gi_sem).wait()


def per_device(nz, x_later, x_earlier, cot_hidden, w_gate, w_up, grad_gate, grad_up):
    rows, width = x_later.shape
    steps = nz // 4
    dma = pltpu.SemaphoreType.DMA
    vmem = pltpu.VMEM
    hid, gi, ngg, ngu = pl.pallas_call(
        functools.partial(kernel, nz),
        out_shape=(
            vmem((rows, 128), BF16),
            vmem((nz, rows, 128), BF16),
            vmem((128, 128), F32),
            vmem((128, 128), F32),
        ),
        in_specs=[pl.BlockSpec(memory_space=pl.ANY)] * 7,
        out_specs=(pl.BlockSpec(memory_space=vmem),) * 4,
        scratch_shapes=[
            vmem((rows, width), BF16),
            vmem((rows, width), BF16),
            vmem((2, rows, 128), BF16),
            vmem((128, 128), F32),
            vmem((128, 128), F32),
            vmem((4, 16, 32, 512), BF16),
            vmem((width, 512), BF16),
            vmem((rows, 512), BF16),
            vmem((16, 512, 128), BF16),
            vmem((16, 256, 128), BF16),
            vmem((rows, 128), BF16),
            vmem((nz, rows, 128), F32),
            vmem((2, 2, steps, rows, 128), BF16),
            vmem((2, 2, steps, rows, 128), BF16),
            dma((6,)),
            dma((3,)),
            dma((3,)),
            dma,
            dma((4, 4)),
            dma((2,)),
            dma((2,)),
            dma((2,)),
            dma((16,)),
            dma,
            dma,
            dma,
            dma((SUB, 2, 2, steps)),
            dma,
            dma((SUB, 2, 2, steps)),
            dma,
            dma((SUB,)),
        ],
        compiler_params=pltpu.CompilerParams(
            collective_id=0, has_side_effects=True, vmem_limit_bytes=48 * 1024 * 1024
        ),
        name="step",
    )(
        *(
            pltpu.with_memory_space_constraint(operand, pltpu.HBM)
            for operand in (
                x_later,
                x_earlier,
                cot_hidden,
                w_gate.reshape(4, 32, 128),
                w_up.reshape(4, 32, 128),
                grad_gate,
                grad_up,
            )
        )
    )
    any_spec = pl.BlockSpec(memory_space=pl.ANY)
    return pl.pallas_call(
        store,
        out_shape=(
            jax.ShapeDtypeStruct((rows, 128), BF16),
            jax.ShapeDtypeStruct((rows, width), BF16),
            jax.ShapeDtypeStruct((128, 128), F32),
            jax.ShapeDtypeStruct((128, 128), F32),
        ),
        in_specs=[pl.BlockSpec(memory_space=vmem)] * 4,
        out_specs=(any_spec,) * 4,
        scratch_shapes=[dma, dma, dma, dma],
        name="store",
    )(*(pltpu.with_memory_space_constraint(r, vmem) for r in (hid, gi, ngg, ngu)))


def solution(mesh):
    placed = (
        P("fs", None),
        P("fs", None),
        P("fs", "tp"),
        P("fs", "tp"),
        P("fs", "tp"),
        P("fs", "tp"),
        P("fs", "tp"),
    )
    return jax.shard_map(
        functools.partial(per_device, mesh.shape["tp"] // 2),
        mesh=mesh,
        in_specs=placed,
        out_specs=(P("fs", "tp"), P("fs", None), P("fs", "tp"), P("fs", "tp")),
        check_vma=False,
    )
```

```python
import functools

import jax
import jax.numpy as jnp
from jax import lax
from jax.experimental import pallas as pl
from jax.experimental.pallas import tpu as pltpu
from jax.sharding import PartitionSpec as P

MESH = pl.DeviceIdType.MESH
SUB = 4
DOWN = (8, 6, 4, 2, 0)
UP = (0, 2, 4, 6, 8)
F32 = jnp.float32
BF16 = jnp.bfloat16


def copy_to(src, dst, send_sem, recv_sem, who):
    pltpu.make_async_remote_copy(
        src_ref=src, dst_ref=dst, send_sem=send_sem, recv_sem=recv_sem,
        device_id=who, device_id_type=MESH,
    ).start()


def arrived(ref, sem):
    pltpu.make_async_copy(ref, ref, sem).wait()


def between(stops):
    return [n for n in range(len(stops) - 1) if abs(stops[n] - stops[n + 1]) == 2]


def kernel(
    nz,
    xl_h, xe_h, cot_h, wg_h, wu_h, gg_h, gu_h, hid, gi, ngg, ngu,
    xl, xe, cot, wst, gg, gu,
    wq, wall,
    dcat, dwt, dwr, hid_other,
    pc, ring_s, ring_r,
    in_sem, give_send, give_recv, ag_send, ag_recv,
    share_send, share_recv, dw_send, dw_recv, hid_send, hid_recv,
    rs_send, rs_recv, out_send, out_recv, out_side_recv, d2_send, d2_recv,
):
    rows = xe.shape[0]
    piece = rows // SUB

    f = lax.axis_index("fs")
    t = lax.axis_index("tp")
    y, x = f // 4, f % 4
    z, core = t // 2, t % 2
    x1 = x + 1 - 2 * (x % 2)
    y1 = y + 1 - 2 * (y % 2)
    flips = [y * 4 + x1, y * 4 + (3 - x), y1 * 4 + x, (3 - y) * 4 + x]
    partner = {"fs": f, "tp": z * 2 + 1 - core}

    def across(d, c):
        return {"fs": flips[d % 4], "tp": z * 2 + c}

    def along(by):
        return {"fs": f, "tp": ((z + nz + by) % nz) * 2 + core}

    def at(k):
        return pl.ds(k * piece, piece)

    load_xe = pltpu.make_async_copy(xe_h, xe, in_sem.at[0])
    load_gg = pltpu.make_async_copy(gg_h, gg, in_sem.at[1])
    load_gu = pltpu.make_async_copy(gu_h, gu, in_sem.at[2])
    barrier = pltpu.get_barrier_semaphore()

    def greet(who):
        pl.semaphore_signal(barrier, inc=1, device_id=who, device_id_type=MESH)

    def new_gradients(total):
        load_gg.wait()
        load_gu.wait()
        ngg[...] = gg[...] + jnp.transpose(total[:128])
        ngu[...] = gu[...] + jnp.transpose(total[128:])

    waves = [(1, 1), (2, 1), (3, 1), (4, 2), (6, 2), (8, 8)]

    def wave_of(slot):
        return max(n for n in range(6) if waves[n][0] <= slot)

    @pl.when(core == 0)
    def _():
        load_wg = pltpu.make_async_copy(wg_h, wst.at[0], in_sem.at[3])
        load_wu = pltpu.make_async_copy(wu_h, wst.at[1], in_sem.at[4])
        load_xl = pltpu.make_async_copy(xl_h, xl, in_sem.at[5])
        greet(partner)
        for d in range(4):
            greet(across(d, 1))
        load_wg.start()
        load_wu.start()
        pl.semaphore_wait(barrier, 5)
        load_wg.wait()
        load_wu.wait()
        for s in range(4):
            for q in range(2):
                copy_to(
                    wst.at[q], wq.at[q, 2**s], give_send.at[0], ag_recv.at[wave_of(2**s)],
                    across(q + s, 1),
                )
        for q in range(2):
            copy_to(wst.at[q], wq.at[q, 0], give_send.at[0], give_recv.at[q], partner)
        copy_to(cot_h, cot.at[0], give_send.at[1], give_recv.at[2], partner)
        for load in (load_xe, load_xl, load_gg, load_gu):
            load.start()

        arrived(dcat, share_recv.at[0])
        load_xe.wait()
        turned = jnp.transpose(dcat[...].astype(F32)).astype(BF16)
        for j in range(4):
            block = jnp.dot(turned, xe[:, 512 * j : 512 * j + 512], preferred_element_type=F32)
            for i in range(4):
                dwt[4 * j + i] = block[:, 128 * i : 128 * i + 128].astype(BF16)
        copy_to(dwt.at[f, pl.ds(256, 256)], dwr.at[0], dw_send.at[1], dw_recv, partner)
        for i in range(1, 16):
            to = (f + i) % 16
            for c in range(2):
                copy_to(
                    dwt.at[to, pl.ds(256 * c, 256)], dwr.at[i], dw_send.at[0], dw_recv,
                    {"fs": to, "tp": z * 2 + c},
                )

        load_xl.wait()
        arrived(wall, share_recv.at[1])
        both = jnp.dot(xl[...], wall[...], preferred_element_type=F32)
        gate, upv = both[:, 256:384], both[:, 384:]
        hid_other[...] = (gate * jax.nn.sigmoid(gate) * upv).astype(BF16)
        gate, upv = both[:, :128], both[:, 128:256]
        hid[...] = (gate * jax.nn.sigmoid(gate) * upv).astype(BF16)

        total = dwt[f, pl.ds(0, 256)].astype(F32)
        copy_to(hid_other, hid, hid_send, hid_recv, partner)
        arrived(dwr.at[pl.ds(1, 15)], dw_recv)
        for i in range(1, 16):
            total = total + dwr[i].astype(F32)
        new_gradients(total)

        arrived(gi, d2_recv)
        arrived(wq.at[0, pl.ds(0, 10)], give_send.at[0])
        pltpu.make_async_copy(cot_h, cot_h, give_send.at[1]).wait()
        arrived(hid_other, hid_send)
        arrived(dwt.at[pl.ds(0, 15)], dw_send.at[0])
        arrived(dwr.at[0], dw_send.at[1])

    @pl.when(core == 1)
    def _():
        load_wg = pltpu.make_async_copy(wg_h, wq.at[2, 0], in_sem.at[3])
        load_wu = pltpu.make_async_copy(wu_h, wq.at[3, 0], in_sem.at[4])
        load_cot = pltpu.make_async_copy(cot_h, cot.at[1], in_sem.at[5])
        greet(partner)
        for d in range(4):
            greet(across(d, 0))
            greet(across(d, 1))
        for by in (-2, -1, 1, 2):
            greet(along(by))
        for load in (load_wg, load_wu, load_xe, load_cot, load_gg, load_gu):
            load.start()
        pl.semaphore_wait(barrier, 13)

        def gather_send(q, s, first, count):
            copy_to(
                wq.at[q, pl.ds(first, count)], wq.at[q, pl.ds(first + 2**s, count)],
                ag_send, ag_recv.at[wave_of(first + 2**s)], across(q + s, 1),
            )

        def gather_wait(n):
            arrived(wq.at[:, pl.ds(waves[n][0], waves[n][1])], ag_recv.at[n])

        def in_order(first, count):
            for q in range(4):
                for i in range(first, first + count):
                    bits = [(q + b) % 4 for b in range(4) if (i >> b) & 1]
                    ox = x
                    oy = y
                    if 0 in bits:
                        ox = ox + 1 - 2 * (ox % 2)
                    if 1 in bits:
                        ox = 3 - ox
                    if 2 in bits:
                        oy = oy + 1 - 2 * (oy % 2)
                    if 3 in bits:
                        oy = 3 - oy
                    start = pl.multiple_of((oy * 4 + ox) * 128, 128)
                    wall[pl.ds(start, 128), 128 * q : 128 * q + 128] = wq[q, i]

        load_wg.wait()
        load_wu.wait()
        for s in range(4):
            for q in (2, 3):
                gather_send(q, s, 0, 1)
        for n in range(5):
            gather_wait(n)
            first, count = waves[n]
            for s in range(first.bit_length(), 4):
                for q in range(4):
                    gather_send(q, s, first, count)
        for q in range(2):
            arrived(wq.at[q, 0], give_recv.at[q])
        in_order(0, 8)
        gather_wait(5)
        in_order(8, 8)

        load_xe.wait()
        load_cot.wait()
        arrived(cot.at[0], give_recv.at[2])
        both = jnp.dot(xe[...], wall[...], preferred_element_type=F32)
        for c in range(2):
            gate = both[:, 256 * c : 256 * c + 128]
            upv = both[:, 256 * c + 128 : 256 * c + 256]
            sigma = jax.nn.sigmoid(gate)
            cotangent = cot[c].astype(F32)
            delta_up = cotangent * gate * sigma
            delta_gate = cotangent * upv * sigma * (1.0 + gate * (1.0 - sigma))
            dcat[:, 256 * c : 256 * c + 128] = delta_gate.astype(BF16)
            dcat[:, 256 * c + 128 : 256 * c + 256] = delta_up.astype(BF16)

        def chunk(by):
            return (z + nz + by) % nz

        def partials(offsets):
            rhs = jnp.concatenate(
                [wall[pl.ds(pl.multiple_of(chunk(by) * 128, 128), 128), :] for by in offsets], 0
            )
            block = lax.dot_general(
                dcat[...], rhs, (((1,), (1,)), ((), ())), preferred_element_type=F32
            )
            for i, by in enumerate(offsets):
                pc[by % nz] = block[:, 128 * i : 128 * i + 128]

        ways = (1, -1)

        def length(k, w):
            return 8 if (k + w) % 2 == 0 else 7

        def gathered(value, n, k, w):
            first = 0 if n > 0 and DOWN[n - 1] <= length(k, w) else 1
            count = 2 if n - 1 in between(DOWN) else 1
            if first < count:
                part = ring_r.at[w, n - 1, k, pl.ds(first, count - first)]
                arrived(part, rs_recv.at[k, w, n - 1])
                for kind in range(first, count):
                    value = value + ring_r[w, n - 1, k, kind].astype(F32)
            return value

        def reduce_send(value, n, k, w, kind, hops):
            ring_s[w, n, k, kind] = value.astype(BF16)
            copy_to(
                ring_s.at[w, n, k, kind], ring_r.at[w, n, k, kind],
                rs_send, rs_recv.at[k, w, n], along(ways[w] * hops),
            )

        def reduce_stop(n):
            for k in range(SUB):
                for w in range(2):
                    if DOWN[n] <= length(k, w):
                        value = gathered(pc[ways[w] * DOWN[n] % nz, at(k)], n, k, w)
                        reduce_send(value, n, k, w, 0, DOWN[n] - DOWN[n + 1])
                    if n in between(DOWN):
                        reduce_send(pc[ways[w] * (DOWN[n] - 1) % nz, at(k)], n, k, w, 1, 1)

        partials((8, 7, -7, 6))
        reduce_stop(0)
        partials((-6, 5, -5, 4))
        partials((-4, 3, -3, 2))
        partials((-2, 1, -1, 0))
        copy_to(dcat, dcat, share_send.at[0], share_recv.at[0], partner)
        copy_to(wall, wall, share_send.at[1], share_recv.at[1], partner)
        for n in range(1, len(DOWN) - 1):
            reduce_stop(n)

        def spread(n, k, w, origin):
            part = gi.at[origin, at(k)]
            if n + 1 < len(UP) and UP[n + 1] <= length(k, w):
                copy_to(part, part, out_send, out_recv.at[k, w, n], along(ways[w] * (UP[n + 1] - UP[n])))
            if n in between(UP):
                j = between(UP).index(n)
                copy_to(part, part, out_send, out_side_recv.at[w, j], along(ways[w]))

        def to_partner(part):
            copy_to(part, part, d2_send, d2_recv, partner)

        for k in range(SUB):
            value = pc[0, at(k)]
            for w in range(2):
                value = gathered(value, len(DOWN) - 1, k, w)
            gi[z, at(k)] = value.astype(BF16)
            for w in range(2):
                spread(0, k, w, z)
        to_partner(gi.at[z])

        for n in range(len(UP) - 1):
            for k in range(SUB):
                for w in range(2):
                    if UP[n + 1] <= length(k, w):
                        origin = chunk(-ways[w] * UP[n + 1])
                        arrived(gi.at[origin, at(k)], out_recv.at[k, w, n])
                        spread(n + 1, k, w, origin)
                        to_partner(gi.at[origin, at(k)])
            if n in between(UP):
                j = between(UP).index(n)
                for w in range(2):
                    origin = chunk(-ways[w] * (UP[n] + 1))
                    arrived(gi.at[origin], out_side_recv.at[w, j])
                    to_partner(gi.at[origin])
            if n == len(UP) - 3:
                total = jnp.zeros((256, 128), F32)
                arrived(dwr, dw_recv)
                for j in range(16):
                    total = total + dwr[j].astype(F32)
                new_gradients(total)

        arrived(hid, hid_recv)
        arrived(dcat, share_send.at[0])
        arrived(wall, share_send.at[1])
        arrived(wq.at[:, pl.ds(0, 13)], ag_send)
        arrived(gi, d2_send)
        arrived(gi.at[pl.ds(0, nz - 1)], rs_send)
        arrived(gi.at[pl.ds(0, nz - 1)], out_send)


def store(hid, gi, ngg, ngu, hid_o, gi_o, ngg_o, ngu_o, hid_sem, gi_sem, ngg_sem, ngu_sem):
    for o in range(gi.shape[0]):
        pltpu.make_async_copy(gi.at[o], gi_o.at[:, pl.ds(o * 128, 128)], gi_sem).start()
    small = [
        pltpu.make_async_copy(hid, hid_o, hid_sem),
        pltpu.make_async_copy(ngg, ngg_o, ngg_sem),
        pltpu.make_async_copy(ngu, ngu_o, ngu_sem),
    ]
    for copy in small:
        copy.start()
    for copy in small:
        copy.wait()
    pltpu.make_async_copy(gi, gi, gi_sem).wait()


def per_device(nz, x_later, x_earlier, cot_hidden, w_gate, w_up, grad_gate, grad_up):
    rows, width = x_later.shape
    dma = pltpu.SemaphoreType.DMA
    vmem = pltpu.VMEM
    hid, gi, ngg, ngu = pl.pallas_call(
        functools.partial(kernel, nz),
        out_shape=(
            vmem((rows, 128), BF16),
            vmem((nz, rows, 128), BF16),
            vmem((128, 128), F32),
            vmem((128, 128), F32),
        ),
        in_specs=[pl.BlockSpec(memory_space=pl.ANY)] * 7,
        out_specs=(pl.BlockSpec(memory_space=vmem),) * 4,
        scratch_shapes=[
            vmem((rows, width), BF16),
            vmem((rows, width), BF16),
            vmem((2, rows, 128), BF16),
            vmem((2, 128, 128), BF16),
            vmem((128, 128), F32),
            vmem((128, 128), F32),
            vmem((4, 16, 128, 128), BF16),
            vmem((width, 512), BF16),
            vmem((rows, 512), BF16),
            vmem((16, 512, 128), BF16),
            vmem((16, 256, 128), BF16),
            vmem((rows, 128), BF16),
            vmem((nz, rows, 128), F32),
            vmem((2, len(DOWN) - 1, SUB, 2, rows // SUB, 128), BF16),
            vmem((2, len(DOWN) - 1, SUB, 2, rows // SUB, 128), BF16),
            dma((6,)),
            dma((2,)),
            dma((3,)),
            dma,
            dma((6,)),
            dma((2,)),
            dma((2,)),
            dma((2,)),
            dma,
            dma,
            dma,
            dma,
            dma((SUB, 2, len(DOWN) - 1)),
            dma,
            dma((SUB, 2, len(UP) - 1)),
            dma((2, max(1, len(between(UP))))),
            dma,
            dma,
        ],
        compiler_params=pltpu.CompilerParams(
            collective_id=0, has_side_effects=True, vmem_limit_bytes=48 * 1024 * 1024
        ),
        name="step",
    )(
        *(
            pltpu.with_memory_space_constraint(operand, pltpu.HBM)
            for operand in (
                x_later,
                x_earlier,
                cot_hidden,
                w_gate,
                w_up,
                grad_gate,
                grad_up,
            )
        )
    )
    any_spec = pl.BlockSpec(memory_space=pl.ANY)
    return pl.pallas_call(
        store,
        out_shape=(
            jax.ShapeDtypeStruct((rows, 128), BF16),
            jax.ShapeDtypeStruct((rows, width), BF16),
            jax.ShapeDtypeStruct((128, 128), F32),
            jax.ShapeDtypeStruct((128, 128), F32),
        ),
        in_specs=[pl.BlockSpec(memory_space=vmem)] * 4,
        out_specs=(any_spec,) * 4,
        scratch_shapes=[dma, dma, dma, dma],
        name="store",
    )(*(pltpu.with_memory_space_constraint(r, vmem) for r in (hid, gi, ngg, ngu)))


def solution(mesh):
    placed = (
        P("fs", None),
        P("fs", None),
        P("fs", "tp"),
        P("fs", "tp"),
        P("fs", "tp"),
        P("fs", "tp"),
        P("fs", "tp"),
    )
    return jax.shard_map(
        functools.partial(per_device, mesh.shape["tp"] // 2),
        mesh=mesh,
        in_specs=placed,
        out_specs=(P("fs", "tp"), P("fs", None), P("fs", "tp"), P("fs", "tp")),
        check_vma=False,
    )
```

```python
import functools

import jax
import jax.numpy as jnp
from jax import lax
from jax.experimental import pallas as pl
from jax.experimental.pallas import tpu as pltpu
from jax.sharding import PartitionSpec as P

MESH = pl.DeviceIdType.MESH
SUB = 6
DOWN = (8, 6, 4, 2, 0)
UP = (0, 2, 4, 6, 8)
F32 = jnp.float32
BF16 = jnp.bfloat16


def copy_to(src, dst, send_sem, recv_sem, who):
    pltpu.make_async_remote_copy(
        src_ref=src, dst_ref=dst, send_sem=send_sem, recv_sem=recv_sem,
        device_id=who, device_id_type=MESH,
    ).start()


def arrived(ref, sem):
    pltpu.make_async_copy(ref, ref, sem).wait()


def between(stops):
    return [n for n in range(len(stops) - 1) if abs(stops[n] - stops[n + 1]) == 2]


def kernel(
    nz,
    xl_h, xe_h, cot_h, wg_h, wu_h, gg_h, gu_h, hid, gi, ngg, ngu,
    xl, xe, cot, wst, grads, grads_other,
    wq,
    dcat, dwt, dwr, hid_other,
    pc, ring_s, ring_r,
    in_sem, give_send, give_recv, ag_send, first_recv, second_recv,
    share_send, share_recv, dw_send, dw_recv, hid_send, hid_recv,
    grads_send, grads_recv, new_recv,
    rs_send, rs_recv, out_send, out_recv, out_side_recv, d2_send, d2_recv,
):
    rows = xe.shape[0]
    piece = rows // SUB

    f = lax.axis_index("fs")
    t = lax.axis_index("tp")
    y, x = f // 4, f % 4
    z, core = t // 2, t % 2
    partner = {"fs": f, "tp": z * 2 + 1 - core}

    def beside(d, by, c):
        place = (y * 4 + (x + by) % 4, (y + by) % 4 * 4 + x)[d]
        return {"fs": place, "tp": z * 2 + c}

    def along(by):
        return {"fs": f, "tp": ((z + nz + by) % nz) * 2 + core}

    def at(k):
        return pl.ds(k * piece, piece)

    load_xe = pltpu.make_async_copy(xe_h, xe, in_sem.at[0])
    barrier = pltpu.get_barrier_semaphore()

    def greet(who):
        pl.semaphore_signal(barrier, inc=1, device_id=who, device_id_type=MESH)

    def weights():
        return jnp.concatenate([wq[q].reshape(16 * 128, 128) for q in range(4)], 1)

    @pl.when(core == 0)
    def _():
        load_wg = pltpu.make_async_copy(wg_h, wst.at[0], in_sem.at[3])
        load_wu = pltpu.make_async_copy(wu_h, wst.at[1], in_sem.at[4])
        load_xl = pltpu.make_async_copy(xl_h, xl, in_sem.at[5])
        load_gg = pltpu.make_async_copy(gg_h, grads.at[0], in_sem.at[1])
        load_gu = pltpu.make_async_copy(gu_h, grads.at[1], in_sem.at[2])
        greet(partner)
        load_wg.start()
        load_wu.start()
        pl.semaphore_wait(barrier, 4)
        load_wg.wait()
        load_wu.wait()
        mine = wq.at[pl.ds(0, 2), f]
        for by in (2, 1, 3):
            copy_to(wst, mine, give_send.at[0], first_recv.at[0, by - 1], beside(0, by, 1))
        copy_to(wst, mine, give_send.at[0], give_recv.at[0], partner)
        copy_to(cot_h, cot.at[0], give_send.at[1], give_recv.at[1], partner)
        for load in (load_xe, load_xl, load_gg, load_gu):
            load.start()

        arrived(dcat, share_recv.at[0])
        load_xe.wait()
        turned = jnp.transpose(dcat[...].astype(F32)).astype(BF16)
        for j in range(4):
            block = jnp.dot(turned, xe[:, 512 * j : 512 * j + 512], preferred_element_type=F32)
            for i in range(4):
                dwt[4 * j + i] = block[:, 128 * i : 128 * i + 128].astype(BF16)
        for i in range(1, 16):
            to = (f + i) % 16
            copy_to(
                dwt.at[to], dwr.at[i - 1], dw_send, dw_recv, {"fs": to, "tp": z * 2}
            )

        load_xl.wait()
        arrived(wq, share_recv.at[1])
        both = jnp.dot(xl[...], weights(), preferred_element_type=F32)
        gate, upv = both[:, 256:384], both[:, 384:]
        hid_other[...] = (gate * jax.nn.sigmoid(gate) * upv).astype(BF16)
        gate, upv = both[:, :128], both[:, 128:256]
        hid[...] = (gate * jax.nn.sigmoid(gate) * upv).astype(BF16)

        copy_to(hid_other, hid, hid_send, hid_recv, partner)

        total = dwt[f].astype(F32)
        arrived(dwr, dw_recv)
        for i in range(15):
            total = total + dwr[i].astype(F32)
        arrived(grads.at[pl.ds(2, 2)], grads_recv)
        for i in range(2):
            grads_other[i] = grads[2 + i] + jnp.transpose(total[256 + 128 * i : 384 + 128 * i])
        load_gg.wait()
        load_gu.wait()
        ngg[...] = grads[0] + jnp.transpose(total[:128])
        ngu[...] = grads[1] + jnp.transpose(total[128:256])
        copy_to(grads_other.at[0], ngg, grads_send, new_recv.at[0], partner)
        copy_to(grads_other.at[1], ngu, grads_send, new_recv.at[1], partner)

        arrived(gi, d2_recv)
        arrived(wq.at[pl.ds(0, 2), pl.ds(0, 4)], give_send.at[0])
        pltpu.make_async_copy(cot_h, cot_h, give_send.at[1]).wait()
        arrived(hid_other, hid_send)
        arrived(dwr, dw_send)
        arrived(grads_other, grads_send)

    @pl.when(core == 1)
    def _():
        load_wg = pltpu.make_async_copy(wg_h, wq.at[2, f], in_sem.at[3])
        load_wu = pltpu.make_async_copy(wu_h, wq.at[3, f], in_sem.at[4])
        load_cot = pltpu.make_async_copy(cot_h, cot.at[1], in_sem.at[5])
        greet(partner)
        for by in (1, 2, 3):
            greet(beside(0, by, 0))
            greet(beside(1, by, 1))
        for by in (-2, -1, 1, 2):
            greet(along(by))
        for load in (load_wg, load_wu, load_xe, load_cot):
            load.start()
        pl.semaphore_wait(barrier, 8)

        def block(d, by):
            place = (y * 4 + (x + 4 - by) % 4, (y + 4 - by) % 4 * 4 + x)[d]
            return wq.at[pl.ds(2 * d, 2), place]

        def pass_on(part, d, offsets=(2, 1, 3)):
            for by in offsets:
                copy_to(part, part, ag_send.at[1], second_recv, beside(d, by, 1))

        def come(d, by):
            part = block(d, by)
            arrived(part, first_recv.at[d, by - 1])
            return part

        load_wg.wait()
        load_wu.wait()
        mine = wq.at[pl.ds(2, 2), f]
        for by in (2, 1, 3):
            copy_to(mine, mine, ag_send.at[0], first_recv.at[1, by - 1], beside(1, by, 1))
        arrived(wq.at[pl.ds(0, 2), f], give_recv.at[0])
        pass_on(wq.at[pl.ds(0, 2), f], 1)
        for by in (1, 3):
            pass_on(come(0, by), 1)
            pass_on(mine, 0, (4 - by,))
        for by in (1, 3):
            pass_on(come(1, by), 0, (1, 3))
        pass_on(come(0, 2), 1)
        for part in (mine, block(1, 1), block(1, 3)):
            pass_on(part, 0, (2,))
        pass_on(come(1, 2), 0)
        arrived(wq.at[:, pl.ds(0, 12)], second_recv)

        load_xe.wait()
        load_cot.wait()
        arrived(cot.at[0], give_recv.at[1])
        def deltas(rs):
            both = jnp.dot(xe[rs, :], weights(), preferred_element_type=F32)
            for c in range(2):
                gate = both[:, 256 * c : 256 * c + 128]
                upv = both[:, 256 * c + 128 : 256 * c + 256]
                sigma = jax.nn.sigmoid(gate)
                cotangent = cot[c, rs].astype(F32)
                delta_up = cotangent * gate * sigma
                delta_gate = cotangent * upv * sigma * (1.0 + gate * (1.0 - sigma))
                dcat[rs, 256 * c : 256 * c + 128] = delta_gate.astype(BF16)
                dcat[rs, 256 * c + 128 : 256 * c + 256] = delta_up.astype(BF16)

        def chunk(by):
            return (z + nz + by) % nz

        def partials(offsets, rs):
            rhs = jnp.concatenate(
                [jnp.concatenate([wq[q, chunk(by)] for q in range(4)], 1) for by in offsets], 0
            )
            block = lax.dot_general(
                dcat[rs, :], rhs, (((1,), (1,)), ((), ())), preferred_element_type=F32
            )
            for i, by in enumerate(offsets):
                pc[by % nz, rs] = block[:, 128 * i : 128 * i + 128]

        ways = (1, -1)

        def length(k, w):
            return 8 if (k + w) % 2 == 0 else 7

        def gathered(value, n, k, w):
            first = 0 if n > 0 and DOWN[n - 1] <= length(k, w) else 1
            count = 2 if n - 1 in between(DOWN) else 1
            if first < count:
                part = ring_r.at[w, n - 1, k, pl.ds(first, count - first)]
                arrived(part, rs_recv.at[k, w, n - 1])
                for kind in range(first, count):
                    value = value + ring_r[w, n - 1, k, kind].astype(F32)
            return value

        def reduce_send(value, n, k, w, kind, hops):
            ring_s[w, n, k, kind] = value.astype(BF16)
            copy_to(
                ring_s.at[w, n, k, kind], ring_r.at[w, n, k, kind],
                rs_send, rs_recv.at[k, w, n], along(ways[w] * hops),
            )

        def reduce_stop(n, pieces=range(SUB)):
            for k in pieces:
                for w in range(2):
                    if DOWN[n] <= length(k, w):
                        value = gathered(pc[ways[w] * DOWN[n] % nz, at(k)], n, k, w)
                        reduce_send(value, n, k, w, 0, DOWN[n] - DOWN[n + 1])
                    if n in between(DOWN):
                        reduce_send(pc[ways[w] * (DOWN[n] - 1) % nz, at(k)], n, k, w, 1, 1)

        for h in range(2):
            rs = pl.ds(h * (rows // 2), rows // 2)
            deltas(rs)
            partials((8, 7, -7, 6), rs)
            reduce_stop(0, range(h * (SUB // 2), (h + 1) * (SUB // 2)))
        every = pl.ds(0, rows)
        partials((-6, 5, -5, 4), every)
        partials((-4, 3, -3, 2), every)
        partials((-2, 1, -1, 0), every)
        copy_to(dcat, dcat, share_send.at[0], share_recv.at[0], partner)
        copy_to(gg_h, grads.at[2], give_send.at[0], grads_recv, partner)
        copy_to(gu_h, grads.at[3], give_send.at[1], grads_recv, partner)
        copy_to(wq, wq, share_send.at[1], share_recv.at[1], partner)
        for n in range(1, len(DOWN) - 1):
            reduce_stop(n)

        def spread(n, k, w, origin):
            part = gi.at[origin, at(k)]
            if n + 1 < len(UP) and UP[n + 1] <= length(k, w):
                copy_to(part, part, out_send, out_recv.at[k, w, n], along(ways[w] * (UP[n + 1] - UP[n])))
            if n in between(UP):
                j = between(UP).index(n)
                copy_to(part, part, out_send, out_side_recv.at[w, j], along(ways[w]))

        def to_partner(part):
            copy_to(part, part, d2_send, d2_recv, partner)

        for k in range(SUB):
            value = pc[0, at(k)]
            for w in range(2):
                value = gathered(value, len(DOWN) - 1, k, w)
            gi[z, at(k)] = value.astype(BF16)
            for w in range(2):
                spread(0, k, w, z)
        to_partner(gi.at[z])

        for n in range(len(UP) - 1):
            for k in range(SUB):
                for w in range(2):
                    if UP[n + 1] <= length(k, w):
                        origin = chunk(-ways[w] * UP[n + 1])
                        arrived(gi.at[origin, at(k)], out_recv.at[k, w, n])
                        spread(n + 1, k, w, origin)
                        to_partner(gi.at[origin, at(k)])
            if n in between(UP):
                j = between(UP).index(n)
                for w in range(2):
                    origin = chunk(-ways[w] * (UP[n] + 1))
                    arrived(gi.at[origin], out_side_recv.at[w, j])
                    to_partner(gi.at[origin])

        arrived(hid, hid_recv)
        arrived(ngg, new_recv.at[0])
        arrived(ngu, new_recv.at[1])
        pltpu.make_async_copy(gg_h, gg_h, give_send.at[0]).wait()
        pltpu.make_async_copy(gu_h, gu_h, give_send.at[1]).wait()
        arrived(dcat, share_send.at[0])
        arrived(wq, share_send.at[1])
        arrived(wq.at[pl.ds(0, 2), pl.ds(0, 3)], ag_send.at[0])
        arrived(wq.at[:, pl.ds(0, 12)], ag_send.at[1])
        arrived(gi, d2_send)
        arrived(gi.at[pl.ds(0, nz - 1)], rs_send)
        arrived(gi.at[pl.ds(0, nz - 1)], out_send)


def store(hid, gi, ngg, ngu, hid_o, gi_o, ngg_o, ngu_o, hid_sem, gi_sem, ngg_sem, ngu_sem):
    for o in range(gi.shape[0]):
        pltpu.make_async_copy(gi.at[o], gi_o.at[:, pl.ds(o * 128, 128)], gi_sem).start()
    small = [
        pltpu.make_async_copy(hid, hid_o, hid_sem),
        pltpu.make_async_copy(ngg, ngg_o, ngg_sem),
        pltpu.make_async_copy(ngu, ngu_o, ngu_sem),
    ]
    for copy in small:
        copy.start()
    for copy in small:
        copy.wait()
    pltpu.make_async_copy(gi, gi, gi_sem).wait()


def per_device(nz, x_later, x_earlier, cot_hidden, w_gate, w_up, grad_gate, grad_up):
    rows, width = x_later.shape
    dma = pltpu.SemaphoreType.DMA
    vmem = pltpu.VMEM
    hid, gi, ngg, ngu = pl.pallas_call(
        functools.partial(kernel, nz),
        out_shape=(
            vmem((rows, 128), BF16),
            vmem((nz, rows, 128), BF16),
            vmem((128, 128), F32),
            vmem((128, 128), F32),
        ),
        in_specs=[pl.BlockSpec(memory_space=pl.ANY)] * 7,
        out_specs=(pl.BlockSpec(memory_space=vmem),) * 4,
        scratch_shapes=[
            vmem((rows, width), BF16),
            vmem((rows, width), BF16),
            vmem((2, rows, 128), BF16),
            vmem((2, 128, 128), BF16),
            vmem((4, 128, 128), F32),
            vmem((2, 128, 128), F32),
            vmem((4, 16, 128, 128), BF16),
            vmem((rows, 512), BF16),
            vmem((16, 512, 128), BF16),
            vmem((15, 512, 128), BF16),
            vmem((rows, 128), BF16),
            vmem((nz, rows, 128), F32),
            vmem((2, len(DOWN) - 1, SUB, 2, rows // SUB, 128), BF16),
            vmem((2, len(DOWN) - 1, SUB, 2, rows // SUB, 128), BF16),
            dma((6,)),
            dma((2,)),
            dma((2,)),
            dma((2,)),
            dma((2, 3)),
            dma,
            dma((2,)),
            dma((2,)),
            dma,
            dma,
            dma,
            dma,
            dma,
            dma,
            dma((2,)),
            dma,
            dma((SUB, 2, len(DOWN) - 1)),
            dma,
            dma((SUB, 2, len(UP) - 1)),
            dma((2, max(1, len(between(UP))))),
            dma,
            dma,
        ],
        compiler_params=pltpu.CompilerParams(
            collective_id=0, has_side_effects=True, vmem_limit_bytes=48 * 1024 * 1024
        ),
        name="step",
    )(
        *(
            pltpu.with_memory_space_constraint(operand, pltpu.HBM)
            for operand in (
                x_later,
                x_earlier,
                cot_hidden,
                w_gate,
                w_up,
                grad_gate,
                grad_up,
            )
        )
    )
    any_spec = pl.BlockSpec(memory_space=pl.ANY)
    return pl.pallas_call(
        store,
        out_shape=(
            jax.ShapeDtypeStruct((rows, 128), BF16),
            jax.ShapeDtypeStruct((rows, width), BF16),
            jax.ShapeDtypeStruct((128, 128), F32),
            jax.ShapeDtypeStruct((128, 128), F32),
        ),
        in_specs=[pl.BlockSpec(memory_space=vmem)] * 4,
        out_specs=(any_spec,) * 4,
        scratch_shapes=[dma, dma, dma, dma],
        name="store",
    )(*(pltpu.with_memory_space_constraint(r, vmem) for r in (hid, gi, ngg, ngu)))


def solution(mesh):
    placed = (
        P("fs", None),
        P("fs", None),
        P("fs", "tp"),
        P("fs", "tp"),
        P("fs", "tp"),
        P("fs", "tp"),
        P("fs", "tp"),
    )
    return jax.shard_map(
        functools.partial(per_device, mesh.shape["tp"] // 2),
        mesh=mesh,
        in_specs=placed,
        out_specs=(P("fs", "tp"), P("fs", None), P("fs", "tp"), P("fs", "tp")),
        check_vma=False,
    )
```

```python
import functools

import jax
import jax.numpy as jnp
from jax import lax
from jax.experimental import pallas as pl
from jax.experimental.pallas import tpu as pltpu
from jax.sharding import PartitionSpec as P

MESH = pl.DeviceIdType.MESH
SUB = 8
DOWN = (8, 6, 4, 2, 0)
UP = (0, 2, 4, 6, 8)
F32 = jnp.float32
BF16 = jnp.bfloat16


def copy_to(src, dst, send_sem, recv_sem, who):
    pltpu.make_async_remote_copy(
        src_ref=src, dst_ref=dst, send_sem=send_sem, recv_sem=recv_sem,
        device_id=who, device_id_type=MESH,
    ).start()


def arrived(ref, sem):
    pltpu.make_async_copy(ref, ref, sem).wait()


def between(stops):
    return [n for n in range(len(stops) - 1) if abs(stops[n] - stops[n + 1]) == 2]


def kernel(
    nz,
    xl_h, xe_h, cot_h, wg_h, wu_h, gg_h, gu_h, hid, gi, ngg, ngu,
    xl, xe, cot, wst, grads, grads_other,
    wq,
    dcat, dwt, dwr, hid_other,
    pc, ring_s, ring_r,
    in_sem, give_send, give_recv, ag_send, first_recv, second_recv,
    share_send, share_recv, dw_send, dw_recv, hid_send, hid_recv,
    grads_send, grads_recv, new_recv,
    rs_send, rs_recv, out_send, out_recv, out_side_recv, d2_send, d2_recv,
):
    rows = xe.shape[0]
    piece = rows // SUB

    f = lax.axis_index("fs")
    t = lax.axis_index("tp")
    y, x = f // 4, f % 4
    z, core = t // 2, t % 2
    partner = {"fs": f, "tp": z * 2 + 1 - core}

    def beside(d, by, c):
        place = (y * 4 + (x + by) % 4, (y + by) % 4 * 4 + x)[d]
        return {"fs": place, "tp": z * 2 + c}

    def along(by):
        return {"fs": f, "tp": ((z + nz + by) % nz) * 2 + core}

    def at(k):
        return pl.ds(k * piece, piece)

    load_xe = pltpu.make_async_copy(xe_h, xe, in_sem.at[0])
    barrier = pltpu.get_barrier_semaphore()

    def greet(who):
        pl.semaphore_signal(barrier, inc=1, device_id=who, device_id_type=MESH)

    def weights():
        return jnp.concatenate([wq[q].reshape(16 * 128, 128) for q in range(4)], 1)

    @pl.when(core == 0)
    def _():
        load_wg = pltpu.make_async_copy(wg_h, wst.at[0], in_sem.at[3])
        load_wu = pltpu.make_async_copy(wu_h, wst.at[1], in_sem.at[4])
        load_xl = pltpu.make_async_copy(xl_h, xl, in_sem.at[5])
        load_gg = pltpu.make_async_copy(gg_h, grads.at[0], in_sem.at[1])
        load_gu = pltpu.make_async_copy(gu_h, grads.at[1], in_sem.at[2])
        greet(partner)
        load_wg.start()
        load_wu.start()
        pl.semaphore_wait(barrier, 4)
        load_wg.wait()
        load_wu.wait()
        mine = wq.at[pl.ds(0, 2), f]
        for by in (2, 1, 3):
            copy_to(wst, mine, give_send.at[0], first_recv.at[0, by - 1], beside(0, by, 1))
        copy_to(wst, mine, give_send.at[0], give_recv.at[0], partner)
        copy_to(cot_h, cot.at[0], give_send.at[1], give_recv.at[1], partner)
        for load in (load_xe, load_xl, load_gg, load_gu):
            load.start()

        arrived(dcat, share_recv.at[0])
        load_xe.wait()
        turned = jnp.transpose(dcat[...].astype(F32)).astype(BF16)
        for j in range(4):
            block = jnp.dot(turned, xe[:, 512 * j : 512 * j + 512], preferred_element_type=F32)
            for i in range(4):
                dwt[4 * j + i] = block[:, 128 * i : 128 * i + 128].astype(BF16)
        for i in range(1, 16):
            to = (f + i) % 16
            copy_to(
                dwt.at[to], dwr.at[i - 1], dw_send, dw_recv, {"fs": to, "tp": z * 2}
            )

        load_xl.wait()
        arrived(wq, share_recv.at[1])
        both = jnp.dot(xl[...], weights(), preferred_element_type=F32)
        gate, upv = both[:, 256:384], both[:, 384:]
        hid_other[...] = (gate * jax.nn.sigmoid(gate) * upv).astype(BF16)
        gate, upv = both[:, :128], both[:, 128:256]
        hid[...] = (gate * jax.nn.sigmoid(gate) * upv).astype(BF16)

        copy_to(hid_other, hid, hid_send, hid_recv, partner)

        total = dwt[f].astype(F32)
        arrived(dwr, dw_recv)
        for i in range(15):
            total = total + dwr[i].astype(F32)
        arrived(grads.at[pl.ds(2, 2)], grads_recv)
        for i in range(2):
            grads_other[i] = grads[2 + i] + jnp.transpose(total[256 + 128 * i : 384 + 128 * i])
        load_gg.wait()
        load_gu.wait()
        ngg[...] = grads[0] + jnp.transpose(total[:128])
        ngu[...] = grads[1] + jnp.transpose(total[128:256])
        copy_to(grads_other.at[0], ngg, grads_send, new_recv.at[0], partner)
        copy_to(grads_other.at[1], ngu, grads_send, new_recv.at[1], partner)

        arrived(gi, d2_recv)
        arrived(wq.at[pl.ds(0, 2), pl.ds(0, 4)], give_send.at[0])
        pltpu.make_async_copy(cot_h, cot_h, give_send.at[1]).wait()
        arrived(hid_other, hid_send)
        arrived(dwr, dw_send)
        arrived(grads_other, grads_send)

    @pl.when(core == 1)
    def _():
        load_wg = pltpu.make_async_copy(wg_h, wq.at[2, f], in_sem.at[3])
        load_wu = pltpu.make_async_copy(wu_h, wq.at[3, f], in_sem.at[4])
        load_cot = pltpu.make_async_copy(cot_h, cot.at[1], in_sem.at[5])
        greet(partner)
        for by in (1, 2, 3):
            greet(beside(0, by, 0))
            greet(beside(1, by, 1))
        for by in (-2, -1, 1, 2):
            greet(along(by))
        for load in (load_wg, load_wu, load_xe, load_cot):
            load.start()
        pl.semaphore_wait(barrier, 8)

        def block(d, by):
            place = (y * 4 + (x + 4 - by) % 4, (y + 4 - by) % 4 * 4 + x)[d]
            return wq.at[pl.ds(2 * d, 2), place]

        def pass_on(part, d, offsets=(2, 1, 3)):
            for by in offsets:
                copy_to(part, part, ag_send.at[1], second_recv, beside(d, by, 1))

        def come(d, by):
            part = block(d, by)
            arrived(part, first_recv.at[d, by - 1])
            return part

        load_wg.wait()
        load_wu.wait()
        mine = wq.at[pl.ds(2, 2), f]
        for by in (2, 1, 3):
            copy_to(mine, mine, ag_send.at[0], first_recv.at[1, by - 1], beside(1, by, 1))
        arrived(wq.at[pl.ds(0, 2), f], give_recv.at[0])
        pass_on(wq.at[pl.ds(0, 2), f], 1)
        for by in (1, 3):
            pass_on(come(0, by), 1)
            pass_on(mine, 0, (4 - by,))
        for by in (1, 3):
            pass_on(come(1, by), 0, (1, 3))
        pass_on(come(0, 2), 1)
        for part in (mine, block(1, 1), block(1, 3)):
            pass_on(part, 0, (2,))
        pass_on(come(1, 2), 0)
        arrived(wq.at[:, pl.ds(0, 12)], second_recv)

        load_xe.wait()
        load_cot.wait()
        arrived(cot.at[0], give_recv.at[1])
        def deltas(rs):
            both = jnp.dot(xe[rs, :], weights(), preferred_element_type=F32)
            for c in range(2):
                gate = both[:, 256 * c : 256 * c + 128]
                upv = both[:, 256 * c + 128 : 256 * c + 256]
                sigma = jax.nn.sigmoid(gate)
                cotangent = cot[c, rs].astype(F32)
                delta_up = cotangent * gate * sigma
                delta_gate = cotangent * upv * sigma * (1.0 + gate * (1.0 - sigma))
                dcat[rs, 256 * c : 256 * c + 128] = delta_gate.astype(BF16)
                dcat[rs, 256 * c + 128 : 256 * c + 256] = delta_up.astype(BF16)

        def chunk(by):
            return (z + nz + by) % nz

        def partials(offsets, rs):
            rhs = jnp.concatenate(
                [jnp.concatenate([wq[q, chunk(by)] for q in range(4)], 1) for by in offsets], 0
            )
            block = lax.dot_general(
                dcat[rs, :], rhs, (((1,), (1,)), ((), ())), preferred_element_type=F32
            )
            for i, by in enumerate(offsets):
                pc[by % nz, rs] = block[:, 128 * i : 128 * i + 128]

        ways = (1, -1)

        def length(k, w):
            return 8 if (k + w) % 2 == 0 else 7

        def gathered(value, n, k, w):
            first = 0 if n > 0 and DOWN[n - 1] <= length(k, w) else 1
            count = 2 if n - 1 in between(DOWN) else 1
            if first < count:
                part = ring_r.at[w, n - 1, k, pl.ds(first, count - first)]
                arrived(part, rs_recv.at[k, w, n - 1])
                for kind in range(first, count):
                    value = value + ring_r[w, n - 1, k, kind].astype(F32)
            return value

        def reduce_send(value, n, k, w, kind, hops):
            ring_s[w, n, k, kind] = value.astype(BF16)
            copy_to(
                ring_s.at[w, n, k, kind], ring_r.at[w, n, k, kind],
                rs_send, rs_recv.at[k, w, n], along(ways[w] * hops),
            )

        def reduce_stop(n, pieces=range(SUB)):
            for k in pieces:
                for w in range(2):
                    if DOWN[n] <= length(k, w):
                        value = gathered(pc[ways[w] * DOWN[n] % nz, at(k)], n, k, w)
                        reduce_send(value, n, k, w, 0, DOWN[n] - DOWN[n + 1])
                    if n in between(DOWN):
                        reduce_send(pc[ways[w] * (DOWN[n] - 1) % nz, at(k)], n, k, w, 1, 1)

        for h in range(2):
            rs = pl.ds(h * (rows // 2), rows // 2)
            deltas(rs)
            partials((8, 7, -7, 6), rs)
            reduce_stop(0, range(h * (SUB // 2), (h + 1) * (SUB // 2)))
        every = pl.ds(0, rows)
        partials((-6, 5, -5, 4), every)
        partials((-4, 3, -3, 2), every)
        partials((-2, 1, -1, 0), every)
        copy_to(dcat, dcat, share_send.at[0], share_recv.at[0], partner)
        copy_to(gg_h, grads.at[2], give_send.at[0], grads_recv, partner)
        copy_to(gu_h, grads.at[3], give_send.at[1], grads_recv, partner)
        copy_to(wq, wq, share_send.at[1], share_recv.at[1], partner)
        for n in range(1, len(DOWN) - 1):
            reduce_stop(n)

        def out_sem(k, w, n):
            return rs_recv.at[k, 1 - w, 2 - n] if n < 3 else out_recv.at[k]

        def spread(n, k, w, origin):
            part = gi.at[origin, at(k)]
            if n + 1 < len(UP) and UP[n + 1] <= length(k, w):
                copy_to(part, part, out_send, out_sem(k, w, n), along(ways[w] * (UP[n + 1] - UP[n])))
            if n in between(UP):
                j = between(UP).index(n)
                copy_to(part, part, out_send, out_side_recv.at[w, j], along(ways[w]))

        def to_partner(part):
            copy_to(part, part, d2_send, d2_recv, partner)

        for k in range(SUB):
            value = pc[0, at(k)]
            for w in range(2):
                value = gathered(value, len(DOWN) - 1, k, w)
            gi[z, at(k)] = value.astype(BF16)
            for w in range(2):
                spread(0, k, w, z)
        to_partner(gi.at[z])

        for n in range(len(UP) - 1):
            for k in range(SUB):
                for w in range(2):
                    if UP[n + 1] <= length(k, w):
                        origin = chunk(-ways[w] * UP[n + 1])
                        arrived(gi.at[origin, at(k)], out_sem(k, w, n))
                        spread(n + 1, k, w, origin)
                        to_partner(gi.at[origin, at(k)])
            if n in between(UP):
                j = between(UP).index(n)
                for w in range(2):
                    origin = chunk(-ways[w] * (UP[n] + 1))
                    arrived(gi.at[origin], out_side_recv.at[w, j])
                    to_partner(gi.at[origin])

        arrived(hid, hid_recv)
        arrived(ngg, new_recv.at[0])
        arrived(ngu, new_recv.at[1])
        pltpu.make_async_copy(gg_h, gg_h, give_send.at[0]).wait()
        pltpu.make_async_copy(gu_h, gu_h, give_send.at[1]).wait()
        arrived(dcat, share_send.at[0])
        arrived(wq, share_send.at[1])
        arrived(wq.at[pl.ds(0, 2), pl.ds(0, 3)], ag_send.at[0])
        arrived(wq.at[:, pl.ds(0, 12)], ag_send.at[1])
        arrived(gi, d2_send)
        arrived(gi.at[pl.ds(0, nz - 1)], rs_send)
        arrived(gi.at[pl.ds(0, nz - 1)], out_send)


def store(hid, gi, ngg, ngu, hid_o, gi_o, ngg_o, ngu_o, hid_sem, gi_sem, ngg_sem, ngu_sem):
    for o in range(gi.shape[0]):
        pltpu.make_async_copy(gi.at[o], gi_o.at[:, pl.ds(o * 128, 128)], gi_sem).start()
    small = [
        pltpu.make_async_copy(hid, hid_o, hid_sem),
        pltpu.make_async_copy(ngg, ngg_o, ngg_sem),
        pltpu.make_async_copy(ngu, ngu_o, ngu_sem),
    ]
    for copy in small:
        copy.start()
    for copy in small:
        copy.wait()
    pltpu.make_async_copy(gi, gi, gi_sem).wait()


def per_device(nz, x_later, x_earlier, cot_hidden, w_gate, w_up, grad_gate, grad_up):
    rows, width = x_later.shape
    dma = pltpu.SemaphoreType.DMA
    vmem = pltpu.VMEM
    hid, gi, ngg, ngu = pl.pallas_call(
        functools.partial(kernel, nz),
        out_shape=(
            vmem((rows, 128), BF16),
            vmem((nz, rows, 128), BF16),
            vmem((128, 128), F32),
            vmem((128, 128), F32),
        ),
        in_specs=[pl.BlockSpec(memory_space=pl.ANY)] * 7,
        out_specs=(pl.BlockSpec(memory_space=vmem),) * 4,
        scratch_shapes=[
            vmem((rows, width), BF16),
            vmem((rows, width), BF16),
            vmem((2, rows, 128), BF16),
            vmem((2, 128, 128), BF16),
            vmem((4, 128, 128), F32),
            vmem((2, 128, 128), F32),
            vmem((4, 16, 128, 128), BF16),
            vmem((rows, 512), BF16),
            vmem((16, 512, 128), BF16),
            vmem((15, 512, 128), BF16),
            vmem((rows, 128), BF16),
            vmem((nz, rows, 128), F32),
            vmem((2, len(DOWN) - 1, SUB, 2, rows // SUB, 128), BF16),
            vmem((2, len(DOWN) - 1, SUB, 2, rows // SUB, 128), BF16),
            dma((6,)),
            dma((2,)),
            dma((2,)),
            dma((2,)),
            dma((2, 3)),
            dma,
            dma((2,)),
            dma((2,)),
            dma,
            dma,
            dma,
            dma,
            dma,
            dma,
            dma((2,)),
            dma,
            dma((SUB, 2, len(DOWN) - 1)),
            dma,
            dma((SUB,)),
            dma((2, max(1, len(between(UP))))),
            dma,
            dma,
        ],
        compiler_params=pltpu.CompilerParams(
            collective_id=0, has_side_effects=True, vmem_limit_bytes=48 * 1024 * 1024
        ),
        name="step",
    )(
        *(
            pltpu.with_memory_space_constraint(operand, pltpu.HBM)
            for operand in (
                x_later,
                x_earlier,
                cot_hidden,
                w_gate,
                w_up,
                grad_gate,
                grad_up,
            )
        )
    )
    any_spec = pl.BlockSpec(memory_space=pl.ANY)
    return pl.pallas_call(
        store,
        out_shape=(
            jax.ShapeDtypeStruct((rows, 128), BF16),
            jax.ShapeDtypeStruct((rows, width), BF16),
            jax.ShapeDtypeStruct((128, 128), F32),
            jax.ShapeDtypeStruct((128, 128), F32),
        ),
        in_specs=[pl.BlockSpec(memory_space=vmem)] * 4,
        out_specs=(any_spec,) * 4,
        scratch_shapes=[dma, dma, dma, dma],
        name="store",
    )(*(pltpu.with_memory_space_constraint(r, vmem) for r in (hid, gi, ngg, ngu)))


def solution(mesh):
    placed = (
        P("fs", None),
        P("fs", None),
        P("fs", "tp"),
        P("fs", "tp"),
        P("fs", "tp"),
        P("fs", "tp"),
        P("fs", "tp"),
    )
    return jax.shard_map(
        functools.partial(per_device, mesh.shape["tp"] // 2),
        mesh=mesh,
        in_specs=placed,
        out_specs=(P("fs", "tp"), P("fs", None), P("fs", "tp"), P("fs", "tp")),
        check_vma=False,
    )
```

```python
import functools

import jax
import jax.numpy as jnp
from jax import lax
from jax.experimental import pallas as pl
from jax.experimental.pallas import tpu as pltpu
from jax.sharding import PartitionSpec as P

MESH = pl.DeviceIdType.MESH
SUB = 8
DOWN = (8, 6, 4, 2, 0)
UP = (0, 2, 4, 6, 8)
F32 = jnp.float32
BF16 = jnp.bfloat16


def copy_to(src, dst, send_sem, recv_sem, who):
    pltpu.make_async_remote_copy(
        src_ref=src, dst_ref=dst, send_sem=send_sem, recv_sem=recv_sem,
        device_id=who, device_id_type=MESH,
    ).start()


def arrived(ref, sem):
    pltpu.make_async_copy(ref, ref, sem).wait()


def between(stops):
    return [n for n in range(len(stops) - 1) if abs(stops[n] - stops[n + 1]) == 2]


def kernel(
    nz,
    xl_h, xe_h, cot_h, wg_h, wu_h, gg_h, gu_h, hid, gi, ngg, ngu,
    xl, xe, cot, wst, grads, grads_other,
    wq,
    dcat, dwt, dwr, hid_other,
    pc, ring_s, ring_r,
    in_sem, give_send, give_recv, ag_send, first_recv, second_recv,
    share_send, share_recv, dw_send, dw_recv, hid_send, hid_recv,
    grads_send, grads_recv, new_recv,
    rs_send, rs_recv, out_send, out_recv, out_side_recv, d2_send, d2_recv,
):
    rows = xe.shape[0]
    piece = rows // SUB

    f = lax.axis_index("fs")
    t = lax.axis_index("tp")
    y, x = f // 4, f % 4
    z, core = t // 2, t % 2
    partner = {"fs": f, "tp": z * 2 + 1 - core}

    def beside(d, by, c):
        place = (y * 4 + (x + by) % 4, (y + by) % 4 * 4 + x)[d]
        return {"fs": place, "tp": z * 2 + c}

    def along(by):
        return {"fs": f, "tp": ((z + nz + by) % nz) * 2 + core}

    def at(k):
        return pl.ds(k * piece, piece)

    load_xe = pltpu.make_async_copy(xe_h, xe, in_sem.at[0])
    barrier = pltpu.get_barrier_semaphore()

    def greet(who):
        pl.semaphore_signal(barrier, inc=1, device_id=who, device_id_type=MESH)

    def weights():
        return jnp.concatenate([wq[q].reshape(16 * 128, 128) for q in range(4)], 1)

    @pl.when(core == 0)
    def _():
        load_wg = pltpu.make_async_copy(wg_h, wst.at[0], in_sem.at[3])
        load_wu = pltpu.make_async_copy(wu_h, wst.at[1], in_sem.at[4])
        load_xl = pltpu.make_async_copy(xl_h, xl, in_sem.at[5])
        load_gg = pltpu.make_async_copy(gg_h, grads.at[0], in_sem.at[1])
        load_gu = pltpu.make_async_copy(gu_h, grads.at[1], in_sem.at[2])
        greet(partner)
        load_wg.start()
        load_wu.start()
        pl.semaphore_wait(barrier, 4)
        load_wg.wait()
        load_wu.wait()
        mine = wq.at[pl.ds(0, 2), f]
        for by in (2, 1, 3):
            copy_to(wst, mine, give_send.at[0], first_recv.at[0, by - 1], beside(0, by, 1))
        copy_to(wst, mine, give_send.at[0], give_recv.at[0], partner)
        copy_to(cot_h, cot.at[0], give_send.at[1], give_recv.at[1], partner)
        for load in (load_xe, load_xl, load_gg, load_gu):
            load.start()

        arrived(dcat, share_recv.at[0])
        load_xe.wait()
        turned = jnp.transpose(dcat[...].astype(F32)).astype(BF16)
        for j in range(4):
            block = jnp.dot(turned, xe[:, 512 * j : 512 * j + 512], preferred_element_type=F32)
            for i in range(4):
                dwt[4 * j + i] = block[:, 128 * i : 128 * i + 128].astype(BF16)
        for i in range(1, 16):
            to = (f + i) % 16
            copy_to(
                dwt.at[to], dwr.at[i - 1], dw_send, dw_recv, {"fs": to, "tp": z * 2}
            )

        load_xl.wait()
        arrived(wq, share_recv.at[1])
        both = jnp.dot(xl[...], weights(), preferred_element_type=F32)
        gate, upv = both[:, 256:384], both[:, 384:]
        hid_other[...] = (gate * jax.nn.sigmoid(gate) * upv).astype(BF16)
        gate, upv = both[:, :128], both[:, 128:256]
        hid[...] = (gate * jax.nn.sigmoid(gate) * upv).astype(BF16)

        copy_to(hid_other, hid, hid_send, hid_recv, partner)

        total = dwt[f].astype(F32)
        arrived(dwr, dw_recv)
        for i in range(15):
            total = total + dwr[i].astype(F32)
        arrived(grads.at[pl.ds(2, 2)], grads_recv)
        for i in range(2):
            grads_other[i] = grads[2 + i] + jnp.transpose(total[256 + 128 * i : 384 + 128 * i])
        load_gg.wait()
        load_gu.wait()
        ngg[...] = grads[0] + jnp.transpose(total[:128])
        ngu[...] = grads[1] + jnp.transpose(total[128:256])
        copy_to(grads_other.at[0], ngg, grads_send, new_recv.at[0], partner)
        copy_to(grads_other.at[1], ngu, grads_send, new_recv.at[1], partner)

        arrived(gi, d2_recv)
        arrived(wq.at[pl.ds(0, 2), pl.ds(0, 4)], give_send.at[0])
        pltpu.make_async_copy(cot_h, cot_h, give_send.at[1]).wait()
        arrived(hid_other, hid_send)
        arrived(dwr, dw_send)
        arrived(grads_other, grads_send)

    @pl.when(core == 1)
    def _():
        load_wg = pltpu.make_async_copy(wg_h, wq.at[2, f], in_sem.at[3])
        load_wu = pltpu.make_async_copy(wu_h, wq.at[3, f], in_sem.at[4])
        load_cot = pltpu.make_async_copy(cot_h, cot.at[1], in_sem.at[5])
        greet(partner)
        for by in (1, 2, 3):
            greet(beside(0, by, 0))
            greet(beside(1, by, 1))
        for by in (-2, -1, 1, 2):
            greet(along(by))
        for load in (load_wg, load_wu, load_xe, load_cot):
            load.start()
        pl.semaphore_wait(barrier, 8)

        def block(d, by):
            place = (y * 4 + (x + 4 - by) % 4, (y + 4 - by) % 4 * 4 + x)[d]
            return wq.at[pl.ds(2 * d, 2), place]

        def pass_on(part, d, offsets=(2, 1, 3)):
            for by in offsets:
                copy_to(part, part, ag_send.at[1], second_recv, beside(d, by, 1))

        def come(d, by):
            part = block(d, by)
            arrived(part, first_recv.at[d, by - 1])
            return part

        load_wg.wait()
        load_wu.wait()
        mine = wq.at[pl.ds(2, 2), f]
        for by in (2, 1, 3):
            copy_to(mine, mine, ag_send.at[0], first_recv.at[1, by - 1], beside(1, by, 1))
        arrived(wq.at[pl.ds(0, 2), f], give_recv.at[0])
        pass_on(wq.at[pl.ds(0, 2), f], 1)
        for by in (1, 3):
            pass_on(come(0, by), 1)
            pass_on(mine, 0, (4 - by,))
        for by in (1, 3):
            pass_on(come(1, by), 0, (1, 3))
        pass_on(come(0, 2), 1)
        for part in (mine, block(1, 1), block(1, 3)):
            pass_on(part, 0, (2,))
        pass_on(come(1, 2), 0)
        arrived(wq.at[:, pl.ds(0, 12)], second_recv)

        load_xe.wait()
        load_cot.wait()
        arrived(cot.at[0], give_recv.at[1])
        def deltas(rs):
            both = jnp.dot(xe[rs, :], weights(), preferred_element_type=F32)
            for c in range(2):
                gate = both[:, 256 * c : 256 * c + 128]
                upv = both[:, 256 * c + 128 : 256 * c + 256]
                sigma = jax.nn.sigmoid(gate)
                cotangent = cot[c, rs].astype(F32)
                delta_up = cotangent * gate * sigma
                delta_gate = cotangent * upv * sigma * (1.0 + gate * (1.0 - sigma))
                dcat[rs, 256 * c : 256 * c + 128] = delta_gate.astype(BF16)
                dcat[rs, 256 * c + 128 : 256 * c + 256] = delta_up.astype(BF16)

        def chunk(by):
            return (z + nz + by) % nz

        def partials(offsets, rs):
            rhs = jnp.concatenate(
                [jnp.concatenate([wq[q, chunk(by)] for q in range(4)], 1) for by in offsets], 0
            )
            block = lax.dot_general(
                dcat[rs, :], rhs, (((1,), (1,)), ((), ())), preferred_element_type=F32
            )
            for i, by in enumerate(offsets):
                pc[by % nz, rs] = block[:, 128 * i : 128 * i + 128]

        ways = (1, -1)

        def length(k, w):
            return 8 if (k + w) % 2 == 0 else 7

        def gathered(value, n, k, w):
            first = 0 if n > 0 and DOWN[n - 1] <= length(k, w) else 1
            count = 2 if n - 1 in between(DOWN) else 1
            if first < count:
                part = ring_r.at[w, n - 1, k, pl.ds(first, count - first)]
                arrived(part, rs_recv.at[k, w, n - 1])
                for kind in range(first, count):
                    value = value + ring_r[w, n - 1, k, kind].astype(F32)
            return value

        def reduce_send(value, n, k, w, kind, hops):
            ring_s[w, n, k, kind] = value.astype(BF16)
            copy_to(
                ring_s.at[w, n, k, kind], ring_r.at[w, n, k, kind],
                rs_send, rs_recv.at[k, w, n], along(ways[w] * hops),
            )

        def reduce_stop(n, pieces=range(SUB)):
            for k in pieces:
                for w in range(2):
                    if DOWN[n] <= length(k, w):
                        value = gathered(pc[ways[w] * DOWN[n] % nz, at(k)], n, k, w)
                        reduce_send(value, n, k, w, 0, DOWN[n] - DOWN[n + 1])
                    if n in between(DOWN):
                        reduce_send(pc[ways[w] * (DOWN[n] - 1) % nz, at(k)], n, k, w, 1, 1)

        for h in range(2):
            rs = pl.ds(h * (rows // 2), rows // 2)
            deltas(rs)
            partials((8, 7, -7, 6), rs)
            reduce_stop(0, range(h * (SUB // 2), (h + 1) * (SUB // 2)))
        every = pl.ds(0, rows)
        partials((-6, 5, -5, 4), every)
        partials((-4, 3, -3, 2), every)
        partials((-2, 1, -1, 0), every)
        copy_to(dcat, dcat, share_send.at[0], share_recv.at[0], partner)
        copy_to(gg_h, grads.at[2], give_send.at[0], grads_recv, partner)
        copy_to(gu_h, grads.at[3], give_send.at[1], grads_recv, partner)
        copy_to(wq, wq, share_send.at[1], share_recv.at[1], partner)
        for n in range(1, len(DOWN) - 1):
            reduce_stop(n)

        def out_sem(k, w, n):
            return rs_recv.at[k, 1 - w, 2 - n] if n < 3 else out_recv.at[k]

        def spread(n, k, w, origin):
            part = gi.at[origin, at(k)]
            if n + 1 < len(UP) and UP[n + 1] <= length(k, w):
                copy_to(part, part, out_send, out_sem(k, w, n), along(ways[w] * (UP[n + 1] - UP[n])))
            if n in between(UP):
                j = between(UP).index(n)
                copy_to(part, part, out_send, out_side_recv.at[w, j], along(ways[w]))

        def to_partner(part):
            copy_to(part, part, d2_send, d2_recv, partner)

        for k in range(SUB):
            value = pc[0, at(k)]
            for w in range(2):
                value = gathered(value, len(DOWN) - 1, k, w)
            gi[z, at(k)] = value.astype(BF16)
            for w in range(2):
                spread(0, k, w, z)
        to_partner(gi.at[z])

        for n in range(len(UP) - 1):
            for k in range(SUB):
                for w in range(2):
                    if UP[n + 1] <= length(k, w):
                        origin = chunk(-ways[w] * UP[n + 1])
                        arrived(gi.at[origin, at(k)], out_sem(k, w, n))
                        spread(n + 1, k, w, origin)
                        if UP[n + 1] == 8:
                            to_partner(gi.at[origin, at(k)])
                        elif k == SUB - 1:
                            to_partner(gi.at[origin])
            if n in between(UP):
                j = between(UP).index(n)
                for w in range(2):
                    origin = chunk(-ways[w] * (UP[n] + 1))
                    arrived(gi.at[origin], out_side_recv.at[w, j])
                    to_partner(gi.at[origin])

        arrived(hid, hid_recv)
        arrived(ngg, new_recv.at[0])
        arrived(ngu, new_recv.at[1])
        pltpu.make_async_copy(gg_h, gg_h, give_send.at[0]).wait()
        pltpu.make_async_copy(gu_h, gu_h, give_send.at[1]).wait()
        arrived(dcat, share_send.at[0])
        arrived(wq, share_send.at[1])
        arrived(wq.at[pl.ds(0, 2), pl.ds(0, 3)], ag_send.at[0])
        arrived(wq.at[:, pl.ds(0, 12)], ag_send.at[1])
        arrived(gi, d2_send)
        arrived(gi.at[pl.ds(0, nz - 1)], rs_send)
        arrived(gi.at[pl.ds(0, nz - 1)], out_send)


def store(hid, gi, ngg, ngu, hid_o, gi_o, ngg_o, ngu_o, hid_sem, gi_sem, ngg_sem, ngu_sem):
    for o in range(gi.shape[0]):
        pltpu.make_async_copy(gi.at[o], gi_o.at[:, pl.ds(o * 128, 128)], gi_sem).start()
    small = [
        pltpu.make_async_copy(hid, hid_o, hid_sem),
        pltpu.make_async_copy(ngg, ngg_o, ngg_sem),
        pltpu.make_async_copy(ngu, ngu_o, ngu_sem),
    ]
    for copy in small:
        copy.start()
    for copy in small:
        copy.wait()
    pltpu.make_async_copy(gi, gi, gi_sem).wait()


def per_device(nz, x_later, x_earlier, cot_hidden, w_gate, w_up, grad_gate, grad_up):
    rows, width = x_later.shape
    dma = pltpu.SemaphoreType.DMA
    vmem = pltpu.VMEM
    hid, gi, ngg, ngu = pl.pallas_call(
        functools.partial(kernel, nz),
        out_shape=(
            vmem((rows, 128), BF16),
            vmem((nz, rows, 128), BF16),
            vmem((128, 128), F32),
            vmem((128, 128), F32),
        ),
        in_specs=[pl.BlockSpec(memory_space=pl.ANY)] * 7,
        out_specs=(pl.BlockSpec(memory_space=vmem),) * 4,
        scratch_shapes=[
            vmem((rows, width), BF16),
            vmem((rows, width), BF16),
            vmem((2, rows, 128), BF16),
            vmem((2, 128, 128), BF16),
            vmem((4, 128, 128), F32),
            vmem((2, 128, 128), F32),
            vmem((4, 16, 128, 128), BF16),
            vmem((rows, 512), BF16),
            vmem((16, 512, 128), BF16),
            vmem((15, 512, 128), BF16),
            vmem((rows, 128), BF16),
            vmem((nz, rows, 128), F32),
            vmem((2, len(DOWN) - 1, SUB, 2, rows // SUB, 128), BF16),
            vmem((2, len(DOWN) - 1, SUB, 2, rows // SUB, 128), BF16),
            dma((6,)),
            dma((2,)),
            dma((2,)),
            dma((2,)),
            dma((2, 3)),
            dma,
            dma((2,)),
            dma((2,)),
            dma,
            dma,
            dma,
            dma,
            dma,
            dma,
            dma((2,)),
            dma,
            dma((SUB, 2, len(DOWN) - 1)),
            dma,
            dma((SUB,)),
            dma((2, max(1, len(between(UP))))),
            dma,
            dma,
        ],
        compiler_params=pltpu.CompilerParams(
            collective_id=0, has_side_effects=True, vmem_limit_bytes=48 * 1024 * 1024
        ),
        name="step",
    )(
        *(
            pltpu.with_memory_space_constraint(operand, pltpu.HBM)
            for operand in (
                x_later,
                x_earlier,
                cot_hidden,
                w_gate,
                w_up,
                grad_gate,
                grad_up,
            )
        )
    )
    any_spec = pl.BlockSpec(memory_space=pl.ANY)
    return pl.pallas_call(
        store,
        out_shape=(
            jax.ShapeDtypeStruct((rows, 128), BF16),
            jax.ShapeDtypeStruct((rows, width), BF16),
            jax.ShapeDtypeStruct((128, 128), F32),
            jax.ShapeDtypeStruct((128, 128), F32),
        ),
        in_specs=[pl.BlockSpec(memory_space=vmem)] * 4,
        out_specs=(any_spec,) * 4,
        scratch_shapes=[dma, dma, dma, dma],
        name="store",
    )(*(pltpu.with_memory_space_constraint(r, vmem) for r in (hid, gi, ngg, ngu)))


def solution(mesh):
    placed = (
        P("fs", None),
        P("fs", None),
        P("fs", "tp"),
        P("fs", "tp"),
        P("fs", "tp"),
        P("fs", "tp"),
        P("fs", "tp"),
    )
    return jax.shard_map(
        functools.partial(per_device, mesh.shape["tp"] // 2),
        mesh=mesh,
        in_specs=placed,
        out_specs=(P("fs", "tp"), P("fs", None), P("fs", "tp"), P("fs", "tp")),
        check_vma=False,
    )
```

```python
import functools

import jax
import jax.numpy as jnp
from jax import lax
from jax.experimental import pallas as pl
from jax.experimental.pallas import tpu as pltpu
from jax.sharding import PartitionSpec as P

MESH = pl.DeviceIdType.MESH
SUB = 8
DOWN = (8, 6, 4, 2, 0)
UP = (0, 2, 4, 6, 8)
F32 = jnp.float32
BF16 = jnp.bfloat16


def copy_to(src, dst, send_sem, recv_sem, who):
    pltpu.make_async_remote_copy(
        src_ref=src, dst_ref=dst, send_sem=send_sem, recv_sem=recv_sem,
        device_id=who, device_id_type=MESH,
    ).start()


def arrived(ref, sem):
    pltpu.make_async_copy(ref, ref, sem).wait()


def between(stops):
    return [n for n in range(len(stops) - 1) if abs(stops[n] - stops[n + 1]) == 2]


def kernel(
    nz,
    xl_h, xe_h, cot_h, wg_h, wu_h, gg_h, gu_h, hid, gi, ngg, ngu,
    xl, xe, cot, wst, grads, grads_other,
    wq,
    dcat, dwt, dwr, hid_other,
    pc, ring_s, ring_r,
    in_sem, give_send, give_recv, ag_send, first_recv, second_recv,
    share_send, share_recv, dw_send, dw_recv, hid_send, hid_recv,
    grads_send, grads_recv, new_recv,
    rs_send, rs_recv, out_send, out_recv, out_side_recv, d2_send, d2_recv,
):
    rows = xe.shape[0]
    piece = rows // SUB

    f = lax.axis_index("fs")
    t = lax.axis_index("tp")
    y, x = f // 4, f % 4
    z, core = t // 2, t % 2
    partner = {"fs": f, "tp": z * 2 + 1 - core}

    def beside(d, by, c):
        place = (y * 4 + (x + by) % 4, (y + by) % 4 * 4 + x)[d]
        return {"fs": place, "tp": z * 2 + c}

    def along(by):
        return {"fs": f, "tp": ((z + nz + by) % nz) * 2 + core}

    def at(k):
        return pl.ds(k * piece, piece)

    load_xe = pltpu.make_async_copy(xe_h, xe, in_sem.at[0])
    barrier = pltpu.get_barrier_semaphore()

    def greet(who):
        pl.semaphore_signal(barrier, inc=1, device_id=who, device_id_type=MESH)

    def weights():
        return jnp.concatenate([wq[q].reshape(16 * 128, 128) for q in range(4)], 1)

    @pl.when(core == 0)
    def _():
        load_wg = pltpu.make_async_copy(wg_h, wst.at[0], in_sem.at[3])
        load_wu = pltpu.make_async_copy(wu_h, wst.at[1], in_sem.at[4])
        load_xl = pltpu.make_async_copy(xl_h, xl, in_sem.at[5])
        load_gg = pltpu.make_async_copy(gg_h, grads.at[0], in_sem.at[1])
        load_gu = pltpu.make_async_copy(gu_h, grads.at[1], in_sem.at[2])
        load_wg.start()
        load_wu.start()
        greet(partner)
        pl.semaphore_wait(barrier, 4)
        load_wg.wait()
        load_wu.wait()
        mine = wq.at[pl.ds(0, 2), f]
        for by in (2, 1, 3):
            copy_to(wst, mine, give_send.at[0], first_recv.at[0, by - 1], beside(0, by, 1))
        copy_to(wst, mine, give_send.at[0], give_recv.at[0], partner)
        copy_to(cot_h, cot.at[0], give_send.at[1], give_recv.at[1], partner)
        for load in (load_xe, load_xl, load_gg, load_gu):
            load.start()

        arrived(dcat, share_recv.at[0])
        load_xe.wait()
        turned = jnp.transpose(dcat[...].astype(F32)).astype(BF16)
        for j in range(4):
            block = jnp.dot(turned, xe[:, 512 * j : 512 * j + 512], preferred_element_type=F32)
            for i in range(4):
                dwt[4 * j + i] = block[:, 128 * i : 128 * i + 128].astype(BF16)
        for i in range(1, 16):
            to = (f + i) % 16
            copy_to(
                dwt.at[to], dwr.at[i - 1], dw_send, dw_recv, {"fs": to, "tp": z * 2}
            )

        load_xl.wait()
        arrived(wq, share_recv.at[1])
        both = jnp.dot(xl[...], weights(), preferred_element_type=F32)
        gate, upv = both[:, 256:384], both[:, 384:]
        hid_other[...] = (gate * jax.nn.sigmoid(gate) * upv).astype(BF16)
        gate, upv = both[:, :128], both[:, 128:256]
        hid[...] = (gate * jax.nn.sigmoid(gate) * upv).astype(BF16)

        copy_to(hid_other, hid, hid_send, hid_recv, partner)

        total = dwt[f].astype(F32)
        arrived(dwr, dw_recv)
        for i in range(15):
            total = total + dwr[i].astype(F32)
        arrived(grads.at[pl.ds(2, 2)], grads_recv)
        for i in range(2):
            grads_other[i] = grads[2 + i] + jnp.transpose(total[256 + 128 * i : 384 + 128 * i])
        load_gg.wait()
        load_gu.wait()
        ngg[...] = grads[0] + jnp.transpose(total[:128])
        ngu[...] = grads[1] + jnp.transpose(total[128:256])
        copy_to(grads_other.at[0], ngg, grads_send, new_recv.at[0], partner)
        copy_to(grads_other.at[1], ngu, grads_send, new_recv.at[1], partner)

        arrived(gi, d2_recv)
        arrived(wq.at[pl.ds(0, 2), pl.ds(0, 4)], give_send.at[0])
        pltpu.make_async_copy(cot_h, cot_h, give_send.at[1]).wait()
        arrived(hid_other, hid_send)
        arrived(dwr, dw_send)
        arrived(grads_other, grads_send)

    @pl.when(core == 1)
    def _():
        load_wg = pltpu.make_async_copy(wg_h, wq.at[2, f], in_sem.at[3])
        load_wu = pltpu.make_async_copy(wu_h, wq.at[3, f], in_sem.at[4])
        load_cot = pltpu.make_async_copy(cot_h, cot.at[1], in_sem.at[5])
        for load in (load_wg, load_wu):
            load.start()
        greet(partner)
        for by in (1, 2, 3):
            greet(beside(0, by, 0))
            greet(beside(1, by, 1))
        for by in (-2, -1, 1, 2):
            greet(along(by))
        for load in (load_xe, load_cot):
            load.start()
        pl.semaphore_wait(barrier, 8)

        def block(d, by):
            place = (y * 4 + (x + 4 - by) % 4, (y + 4 - by) % 4 * 4 + x)[d]
            return wq.at[pl.ds(2 * d, 2), place]

        def pass_on(part, d, offsets=(2, 1, 3)):
            for by in offsets:
                copy_to(part, part, ag_send.at[1], second_recv, beside(d, by, 1))

        def come(d, by):
            part = block(d, by)
            arrived(part, first_recv.at[d, by - 1])
            return part

        load_wg.wait()
        load_wu.wait()
        mine = wq.at[pl.ds(2, 2), f]
        for by in (2, 1, 3):
            copy_to(mine, mine, ag_send.at[0], first_recv.at[1, by - 1], beside(1, by, 1))
        arrived(wq.at[pl.ds(0, 2), f], give_recv.at[0])
        pass_on(wq.at[pl.ds(0, 2), f], 1)
        for by in (1, 3):
            pass_on(come(0, by), 1)
            pass_on(mine, 0, (4 - by,))
        for by in (1, 3):
            pass_on(come(1, by), 0, (1, 3))
        pass_on(come(0, 2), 1)
        for part in (mine, block(1, 1), block(1, 3)):
            pass_on(part, 0, (2,))
        pass_on(come(1, 2), 0)
        arrived(wq.at[:, pl.ds(0, 12)], second_recv)

        load_xe.wait()
        load_cot.wait()
        arrived(cot.at[0], give_recv.at[1])
        def deltas(rs):
            both = jnp.dot(xe[rs, :], weights(), preferred_element_type=F32)
            for c in range(2):
                gate = both[:, 256 * c : 256 * c + 128]
                upv = both[:, 256 * c + 128 : 256 * c + 256]
                sigma = jax.nn.sigmoid(gate)
                cotangent = cot[c, rs].astype(F32)
                delta_up = cotangent * gate * sigma
                delta_gate = cotangent * upv * sigma * (1.0 + gate * (1.0 - sigma))
                dcat[rs, 256 * c : 256 * c + 128] = delta_gate.astype(BF16)
                dcat[rs, 256 * c + 128 : 256 * c + 256] = delta_up.astype(BF16)

        def chunk(by):
            return (z + nz + by) % nz

        def partials(offsets, rs):
            rhs = jnp.concatenate(
                [jnp.concatenate([wq[q, chunk(by)] for q in range(4)], 1) for by in offsets], 0
            )
            block = lax.dot_general(
                dcat[rs, :], rhs, (((1,), (1,)), ((), ())), preferred_element_type=F32
            )
            for i, by in enumerate(offsets):
                pc[by % nz, rs] = block[:, 128 * i : 128 * i + 128]

        ways = (1, -1)

        def length(k, w):
            return 8 if (k + w) % 2 == 0 else 7

        def gathered(value, n, k, w):
            first = 0 if n > 0 and DOWN[n - 1] <= length(k, w) else 1
            count = 2 if n - 1 in between(DOWN) else 1
            if first < count:
                part = ring_r.at[w, n - 1, k, pl.ds(first, count - first)]
                arrived(part, rs_recv.at[k, w, n - 1])
                for kind in range(first, count):
                    value = value + ring_r[w, n - 1, k, kind].astype(F32)
            return value

        def reduce_send(value, n, k, w, kind, hops):
            ring_s[w, n, k, kind] = value.astype(BF16)
            copy_to(
                ring_s.at[w, n, k, kind], ring_r.at[w, n, k, kind],
                rs_send, rs_recv.at[k, w, n], along(ways[w] * hops),
            )

        def reduce_stop(n, pieces=range(SUB)):
            for k in pieces:
                for w in range(2):
                    if DOWN[n] <= length(k, w):
                        value = gathered(pc[ways[w] * DOWN[n] % nz, at(k)], n, k, w)
                        reduce_send(value, n, k, w, 0, DOWN[n] - DOWN[n + 1])
                    if n in between(DOWN):
                        reduce_send(pc[ways[w] * (DOWN[n] - 1) % nz, at(k)], n, k, w, 1, 1)

        for h in range(2):
            rs = pl.ds(h * (rows // 2), rows // 2)
            deltas(rs)
            partials((8, 7, -7, 6), rs)
            reduce_stop(0, range(h * (SUB // 2), (h + 1) * (SUB // 2)))
        every = pl.ds(0, rows)
        partials((-6, 5, -5, 4), every)
        partials((-4, 3, -3, 2), every)
        partials((-2, 1, -1, 0), every)
        copy_to(dcat, dcat, share_send.at[0], share_recv.at[0], partner)
        copy_to(gg_h, grads.at[2], give_send.at[0], grads_recv, partner)
        copy_to(gu_h, grads.at[3], give_send.at[1], grads_recv, partner)
        copy_to(wq, wq, share_send.at[1], share_recv.at[1], partner)
        for n in range(1, len(DOWN) - 1):
            reduce_stop(n)

        def out_sem(k, w, n):
            return rs_recv.at[k, 1 - w, 2 - n] if n < 3 else out_recv.at[k]

        def spread(n, k, w, origin):
            part = gi.at[origin, at(k)]
            if n + 1 < len(UP) and UP[n + 1] <= length(k, w):
                copy_to(part, part, out_send, out_sem(k, w, n), along(ways[w] * (UP[n + 1] - UP[n])))
            if n in between(UP):
                j = between(UP).index(n)
                copy_to(part, part, out_send, out_side_recv.at[w, j], along(ways[w]))

        def to_partner(part):
            copy_to(part, part, d2_send, d2_recv, partner)

        for k in range(SUB):
            value = pc[0, at(k)]
            for w in range(2):
                value = gathered(value, len(DOWN) - 1, k, w)
            gi[z, at(k)] = value.astype(BF16)
            for w in range(2):
                spread(0, k, w, z)
        to_partner(gi.at[z])

        for n in range(len(UP) - 1):
            for k in range(SUB):
                for w in range(2):
                    if UP[n + 1] <= length(k, w):
                        origin = chunk(-ways[w] * UP[n + 1])
                        arrived(gi.at[origin, at(k)], out_sem(k, w, n))
                        spread(n + 1, k, w, origin)
                        if UP[n + 1] == 8:
                            to_partner(gi.at[origin, at(k)])
                        elif k == SUB - 1:
                            to_partner(gi.at[origin])
            if n in between(UP):
                j = between(UP).index(n)
                for w in range(2):
                    origin = chunk(-ways[w] * (UP[n] + 1))
                    arrived(gi.at[origin], out_side_recv.at[w, j])
                    to_partner(gi.at[origin])

        arrived(hid, hid_recv)
        arrived(ngg, new_recv.at[0])
        arrived(ngu, new_recv.at[1])
        pltpu.make_async_copy(gg_h, gg_h, give_send.at[0]).wait()
        pltpu.make_async_copy(gu_h, gu_h, give_send.at[1]).wait()
        arrived(dcat, share_send.at[0])
        arrived(wq, share_send.at[1])
        arrived(wq.at[pl.ds(0, 2), pl.ds(0, 3)], ag_send.at[0])
        arrived(wq.at[:, pl.ds(0, 12)], ag_send.at[1])
        arrived(gi, d2_send)
        arrived(gi.at[pl.ds(0, nz - 1)], rs_send)
        arrived(gi.at[pl.ds(0, nz - 1)], out_send)


def store(hid, gi, ngg, ngu, hid_o, gi_o, ngg_o, ngu_o, hid_sem, gi_sem, ngg_sem, ngu_sem):
    for o in range(gi.shape[0]):
        pltpu.make_async_copy(gi.at[o], gi_o.at[:, pl.ds(o * 128, 128)], gi_sem).start()
    small = [
        pltpu.make_async_copy(hid, hid_o, hid_sem),
        pltpu.make_async_copy(ngg, ngg_o, ngg_sem),
        pltpu.make_async_copy(ngu, ngu_o, ngu_sem),
    ]
    for copy in small:
        copy.start()
    for copy in small:
        copy.wait()
    pltpu.make_async_copy(gi, gi, gi_sem).wait()


def per_device(nz, x_later, x_earlier, cot_hidden, w_gate, w_up, grad_gate, grad_up):
    rows, width = x_later.shape
    dma = pltpu.SemaphoreType.DMA
    vmem = pltpu.VMEM
    hid, gi, ngg, ngu = pl.pallas_call(
        functools.partial(kernel, nz),
        out_shape=(
            vmem((rows, 128), BF16),
            vmem((nz, rows, 128), BF16),
            vmem((128, 128), F32),
            vmem((128, 128), F32),
        ),
        in_specs=[pl.BlockSpec(memory_space=pl.ANY)] * 7,
        out_specs=(pl.BlockSpec(memory_space=vmem),) * 4,
        scratch_shapes=[
            vmem((rows, width), BF16),
            vmem((rows, width), BF16),
            vmem((2, rows, 128), BF16),
            vmem((2, 128, 128), BF16),
            vmem((4, 128, 128), F32),
            vmem((2, 128, 128), F32),
            vmem((4, 16, 128, 128), BF16),
            vmem((rows, 512), BF16),
            vmem((16, 512, 128), BF16),
            vmem((15, 512, 128), BF16),
            vmem((rows, 128), BF16),
            vmem((nz, rows, 128), F32),
            vmem((2, len(DOWN) - 1, SUB, 2, rows // SUB, 128), BF16),
            vmem((2, len(DOWN) - 1, SUB, 2, rows // SUB, 128), BF16),
            dma((6,)),
            dma((2,)),
            dma((2,)),
            dma((2,)),
            dma((2, 3)),
            dma,
            dma((2,)),
            dma((2,)),
            dma,
            dma,
            dma,
            dma,
            dma,
            dma,
            dma((2,)),
            dma,
            dma((SUB, 2, len(DOWN) - 1)),
            dma,
            dma((SUB,)),
            dma((2, max(1, len(between(UP))))),
            dma,
            dma,
        ],
        compiler_params=pltpu.CompilerParams(
            collective_id=0, has_side_effects=True, vmem_limit_bytes=48 * 1024 * 1024
        ),
        name="step",
    )(
        *(
            pltpu.with_memory_space_constraint(operand, pltpu.HBM)
            for operand in (
                x_later,
                x_earlier,
                cot_hidden,
                w_gate,
                w_up,
                grad_gate,
                grad_up,
            )
        )
    )
    any_spec = pl.BlockSpec(memory_space=pl.ANY)
    return pl.pallas_call(
        store,
        out_shape=(
            jax.ShapeDtypeStruct((rows, 128), BF16),
            jax.ShapeDtypeStruct((rows, width), BF16),
            jax.ShapeDtypeStruct((128, 128), F32),
            jax.ShapeDtypeStruct((128, 128), F32),
        ),
        in_specs=[pl.BlockSpec(memory_space=vmem)] * 4,
        out_specs=(any_spec,) * 4,
        scratch_shapes=[dma, dma, dma, dma],
        name="store",
    )(*(pltpu.with_memory_space_constraint(r, vmem) for r in (hid, gi, ngg, ngu)))


def solution(mesh):
    placed = (
        P("fs", None),
        P("fs", None),
        P("fs", "tp"),
        P("fs", "tp"),
        P("fs", "tp"),
        P("fs", "tp"),
        P("fs", "tp"),
    )
    return jax.shard_map(
        functools.partial(per_device, mesh.shape["tp"] // 2),
        mesh=mesh,
        in_specs=placed,
        out_specs=(P("fs", "tp"), P("fs", None), P("fs", "tp"), P("fs", "tp")),
        check_vma=False,
    )
```
